32 devices in a mesh: sp: 4 (over z), fs: 4 (over y, x), tp: 2 (over core).
Axes of the slice: x: 2, y: 2, z: 4, core: 2. Of those that a mesh axis runs over, the one named last changes fastest.
Arguments:
- tokens: bfloat16 [4, 3072, 2048], P('fs', 'sp'), may hold values from -6 to 6
- norm_gain: float32 [2048], replicated, may hold values from 0.1 to 1.9
- query_weight: bfloat16 [2048, 512], P(('sp', 'fs'), 'tp'), may hold values from -0.125 to 0.125
- key_weight: bfloat16 [2048, 512], P(('sp', 'fs'), 'tp'), may hold values from -0.125 to 0.125
- value_weight: bfloat16 [2048, 1024], P(('sp', 'fs'), 'tp'), may hold values from -0.125 to 0.125
- gate_weight: bfloat16 [2048, 1024], P(('sp', 'fs'), 'tp'), may hold values from -0.125 to 0.125
- conv_b_weight: bfloat16 [2048, 1024], P(('sp', 'fs'), 'tp'), may hold values from -0.125 to 0.125
- conv_c_weight: bfloat16 [2048, 1024], P(('sp', 'fs'), 'tp'), may hold values from -0.125 to 0.125
- conv_in_weight: bfloat16 [2048, 1024], P(('sp', 'fs'), 'tp'), may hold values from -0.125 to 0.125
- conv_kernel: float32 [3, 1024], P(None, 'tp'), may hold values from -3.5 to 3.5
- out_ret_weight: bfloat16 [2048, 1024], P(('sp', 'fs'), 'tp'), may hold values from -0.125 to 0.125
- out_conv_weight: bfloat16 [2048, 1024], P(('sp', 'fs'), 'tp'), may hold values from -0.125 to 0.125
- log_decay: float32 [4, 8, 3072], P('fs', 'tp', 'sp'), may hold values from -3 to 0, as said below
Outputs:
- mixed: bfloat16 [4, 3072, 2048], P('fs', ('sp', 'tp'))
The draws below stay inside these ranges and needn't reach their ends.
Inputs may be any that keep to these rules, and one draw needn't show every extreme that they name: log_decay is never positive.
All inputs are finite; a program needn't handle non-finite values.
Results may differ from the reference program's by a relative error of at most 0.02.
Values may be sent and summed in bfloat16 or wider, within the bound.
A program may use at most 64 MiB of HBM per device.

```python
import jax
import jax.numpy as jnp
from jax import lax

MODEL = 2048
MEMORY_CHANNELS = 8
KEY_DIM = 64
VALUE_DIM = 128
CONV_DIM = 1024
CONV_TAPS = 3
BLOCK_LEN = 128
TOK_DEV = 768
SERIES_NUMBER = 4
SERIES_SPAN = 3072
N_TP = 2


def draw_log_decay(key, part):
    lookup_matrix_lines = jax.random.split(jax.random.fold_in(key, 17), 7)
    head_shape = (SERIES_NUMBER, MEMORY_CHANNELS, 1)
    fast_share = 0.5
    is_fast = jax.random.uniform(lookup_matrix_lines[0], head_shape, jnp.float32) < fast_share
    fast_rate = jnp.exp(jax.random.uniform(lookup_matrix_lines[1], head_shape, jnp.float32, jnp.log(0.04), jnp.log(0.1)))
    slow_rate = jnp.exp(jax.random.uniform(lookup_matrix_lines[2], head_shape, jnp.float32, jnp.log(0.1), jnp.log(0.25))) / SERIES_SPAN
    background_frequency = jnp.where(is_fast, fast_rate, slow_rate)
    segment_multiplier = jnp.exp(jax.random.uniform(lookup_matrix_lines[3], (SERIES_NUMBER, MEMORY_CHANNELS, SERIES_SPAN // TOK_DEV), jnp.float32, -0.7, 0.7))
    segment_multiplier = jnp.repeat(segment_multiplier, TOK_DEV, axis=-1)
    noise_magnitude = jax.random.uniform(lookup_matrix_lines[4], (SERIES_NUMBER, MEMORY_CHANNELS, SERIES_SPAN), jnp.float32, 0.4, 1.6)
    spike_places = jax.random.randint(lookup_matrix_lines[5], (SERIES_NUMBER, MEMORY_CHANNELS, 3), 0, SERIES_SPAN)
    spike_magnitude = jnp.log(jax.random.uniform(lookup_matrix_lines[6], (SERIES_NUMBER, MEMORY_CHANNELS, 3), jnp.float32, 0.55, 0.8))
    token_ordinal = jnp.arange(SERIES_SPAN)
    spike_occurrences = jnp.sum(jnp.where(token_ordinal[None, None, :, None] == spike_places[:, :, None, :], spike_magnitude[:, :, None, :], 0.0), axis=-1)
    return (spike_occurrences - background_frequency * segment_multiplier * noise_magnitude).astype(jnp.float32)


def block_levels(rng, extent, pieces, smallest, top_value):
    gain, own = 1.0, jax.random.fold_in(rng, 6)
    for axis_at, shards_of in pieces:
        draws = jnp.exp(jax.random.uniform(jax.random.fold_in(own, axis_at), (shards_of,), jnp.float32, smallest / len(pieces), top_value / len(pieces)))
        gain = gain * jnp.repeat(draws, extent[axis_at] // shards_of).reshape([-1 if axis == axis_at else 1 for axis in range(len(extent))])
    return gain


def noise(stream_key, dims, width, bound, cuts=(), kind=jnp.bfloat16):
    values = jax.random.normal(stream_key, dims, jnp.float32) * width
    if len(cuts) > 0:
        values = block_levels(stream_key, dims, cuts, -0.22, 0.18) * values
    return jnp.clip(values, min=-bound, max=bound).astype(kind)


def setup_inputs(seed: int = 0) -> dict:
    keys = jax.random.split(jax.random.key(seed), 14)
    return {
        "tokens": noise(keys[0], (SERIES_NUMBER, SERIES_SPAN, MODEL), 1.0, 6.0, ((0, 4), (1, 4))),
        "norm_gain": jnp.clip(1.0 + 0.18 * jax.random.normal(keys[1], (MODEL,), jnp.float32), 0.1, 1.9),
        "query_weight": noise(keys[2], (MODEL, MEMORY_CHANNELS * KEY_DIM), MODEL ** -0.5, 0.125, ((0, 16), (1, 2))),
        "key_weight": noise(keys[3], (MODEL, MEMORY_CHANNELS * KEY_DIM), MODEL ** -0.5, 0.125, ((0, 16), (1, 2))),
        "value_weight": noise(keys[4], (MODEL, MEMORY_CHANNELS * VALUE_DIM), MODEL ** -0.5, 0.125, ((0, 16), (1, 2))),
        "gate_weight": noise(keys[5], (MODEL, MEMORY_CHANNELS * VALUE_DIM), MODEL ** -0.5, 0.125, ((0, 16), (1, 2))),
        "conv_b_weight": noise(keys[6], (MODEL, CONV_DIM), MODEL ** -0.5, 0.125, ((0, 16), (1, 2))),
        "conv_c_weight": noise(keys[7], (MODEL, CONV_DIM), MODEL ** -0.5, 0.125, ((0, 16), (1, 2))),
        "conv_in_weight": noise(keys[8], (MODEL, CONV_DIM), MODEL ** -0.5, 0.125, ((0, 16), (1, 2))),
        "conv_kernel": noise(keys[9], (CONV_TAPS, CONV_DIM), CONV_TAPS ** -0.5, 3.5, ((1, 2),), jnp.float32),
        "out_ret_weight": noise(keys[10], (MODEL, MEMORY_CHANNELS * VALUE_DIM), (MEMORY_CHANNELS * VALUE_DIM + CONV_DIM) ** -0.5, 0.125, ((0, 16), (1, 2))),
        "out_conv_weight": noise(keys[11], (MODEL, CONV_DIM), (MEMORY_CHANNELS * VALUE_DIM + CONV_DIM) ** -0.5, 0.125, ((0, 16), (1, 2))),
        "log_decay": draw_log_decay(jax.random.fold_in(keys[13], 71), 0),
    }


EPSILON = 1e-06
ROPE_BASE = 10000.0

def to_half(values):
    return lax.optimization_barrier(values.astype(jnp.bfloat16))

def rotate(values, token_ordinal):
    half_dim = values.shape[-1] // 2
    frequency = 1.0 / ROPE_BASE ** jnp.linspace(0.0, 1.0, half_dim, dtype=jnp.float32)
    angles = token_ordinal[:, None] * frequency[None, :]
    cosine_table = jnp.cos(angles)[:, None, :]
    sine_table = jnp.sin(angles)[:, None, :]
    first = values[..., :half_dim].astype(jnp.float32)
    second = values[..., half_dim:].astype(jnp.float32)
    return jnp.concatenate([first * cosine_table - second * sine_table, first * sine_table + second * cosine_table], axis=-1)

def retention_pass(queries, lookup_matrix_lines, values, decays):
    length, head_count, key_dim = queries.shape
    blocks = length // BLOCK_LEN

    def split_blocks(array):
        shaped = array.reshape(blocks, BLOCK_LEN, head_count, array.shape[-1])
        return jnp.transpose(shaped, (0, 2, 1, 3)).astype(jnp.float32)
    query_blocks = split_blocks(queries)
    key_blocks = split_blocks(lookup_matrix_lines)
    value_blocks = split_blocks(values)
    decay_blocks = jnp.transpose(decays.reshape(head_count, blocks, BLOCK_LEN), (1, 0, 2))
    cumulative = jnp.cumsum(decay_blocks, axis=-1)
    ending = cumulative[..., -1:]
    decay_gaps = cumulative[..., :, None] - cumulative[..., None, :]
    causal = jnp.arange(BLOCK_LEN)[:, None] >= jnp.arange(BLOCK_LEN)[None, :]
    weighting = jnp.where(causal, jnp.exp(jnp.minimum(decay_gaps, 0.0)), 0.0)
    scores = to_half(jnp.einsum('nhid,nhjd->nhij', query_blocks, key_blocks) * weighting).astype(jnp.float32)
    intra_out = jnp.einsum('nhij,nhje->nhie', scores, value_blocks)
    decayed_keys = to_half(key_blocks * jnp.exp(ending - cumulative)[..., None]).astype(jnp.float32)
    decayed_queries = to_half(query_blocks * jnp.exp(cumulative)[..., None]).astype(jnp.float32)
    block_kv = jnp.einsum('nhjd,nhje->nhde', decayed_keys, value_blocks)

    def advance(state_now, step_in):
        kv_block, total = step_in
        return (state_now * jnp.exp(total)[:, None, None] + kv_block, state_now)
    start_state = jnp.zeros((head_count, key_dim, values.shape[-1]), jnp.float32)
    _, before = lax.scan(advance, start_state, (block_kv, ending[..., 0]))
    cross = jnp.einsum('nhid,nhde->nhie', decayed_queries, to_half(before).astype(jnp.float32))
    output = intra_out + cross
    output = output * lax.rsqrt(lax.optimization_barrier(jnp.mean(output * output, axis=-1, keepdims=True)) + EPSILON)
    return jnp.transpose(output, (0, 2, 1, 3)).reshape(length, head_count * output.shape[-1])

def reference(tokens, norm_gain, query_weight, key_weight, value_weight, gate_weight, conv_b_weight, conv_c_weight, conv_in_weight, conv_kernel, out_ret_weight, out_conv_weight, log_decay):

    def one_sequence(pair):
        sequence_tokens, sequence_decay = pair
        inputs = sequence_tokens.astype(jnp.float32)
        length = inputs.shape[0]
        normed = to_half(inputs * lax.rsqrt(lax.optimization_barrier(jnp.mean(inputs * inputs, axis=-1, keepdims=True)) + EPSILON) * norm_gain.astype(jnp.float32))

        def project(weight):
            return to_half(jnp.dot(normed, weight, preferred_element_type=jnp.float32))
        token_ordinal = jnp.arange(length, dtype=jnp.float32)
        query_raw = project(query_weight).reshape(length, MEMORY_CHANNELS, KEY_DIM)
        key_raw = project(key_weight).reshape(length, MEMORY_CHANNELS, KEY_DIM)
        value_proj = project(value_weight).reshape(length, MEMORY_CHANNELS, VALUE_DIM)
        queries = to_half(rotate(query_raw, token_ordinal))
        lookup_matrix_lines = to_half(rotate(key_raw, token_ordinal) * KEY_DIM ** (-0.5))
        retained = retention_pass(queries, lookup_matrix_lines, value_proj, sequence_decay)
        ret_out = to_half(retained * jax.nn.silu(project(gate_weight).astype(jnp.float32)))
        gate_b = project(conv_b_weight).astype(jnp.float32)
        gate_c = project(conv_c_weight).astype(jnp.float32)
        conv_input = project(conv_in_weight).astype(jnp.float32)
        product = gate_c * conv_input
        padded = jnp.concatenate([jnp.zeros((CONV_TAPS - 1, CONV_DIM), jnp.float32), product], axis=0)
        convolved = jnp.zeros((length, CONV_DIM), jnp.float32)
        for tap_index in range(CONV_TAPS):
            convolved = convolved + conv_kernel[tap_index].astype(jnp.float32) * padded[tap_index:tap_index + length]
        conv_out = to_half(gate_b * convolved)
        ret_group = MEMORY_CHANNELS * VALUE_DIM // N_TP
        conv_group = CONV_DIM // N_TP
        total = jnp.zeros((length, MODEL), jnp.float32)
        for group in range(N_TP):
            ret_cols = slice(group * ret_group, (group + 1) * ret_group)
            conv_cols = slice(group * conv_group, (group + 1) * conv_group)
            partial_value = jnp.dot(ret_out[:, ret_cols], out_ret_weight[:, ret_cols].T, preferred_element_type=jnp.float32)
            partial_value = partial_value + jnp.dot(conv_out[:, conv_cols], out_conv_weight[:, conv_cols].T, preferred_element_type=jnp.float32)
            total = total + to_half(partial_value).astype(jnp.float32)
        return total.astype(jnp.bfloat16)
    return lax.map(one_sequence, (tokens, log_decay))
```

```python
import jax
import numpy as np
import jax.numpy as jnp
from jax import lax
from jax.experimental import pallas as pl
from jax.experimental.pallas import tpu as pltpu
from jax.sharding import PartitionSpec as P

KEY_DIM = 64
VALUE_DIM = 128
CONV_TAPS = 3
BLOCK_LEN = 128


EPSILON = 1e-06
ROPE_BASE = 10000.0


def entering(x, axis, combine, identity):
    length, here = (lax.axis_size(axis), lax.axis_index(axis))
    everything = jax.tree.map(
        lambda part, kind: lax.all_gather(part.astype(kind), axis), x, (jnp.bfloat16, jnp.bfloat16)
    )
    start = jax.tree.map(
        lambda part, zero: jnp.broadcast_to(jnp.asarray(zero, part.dtype), part.shape), x, identity
    )

    def lap(k, before):
        reached = k < here
        new = combine(
            before, jax.tree.map(lambda part, own: part[k].astype(own.dtype), everything, x)
        )
        return jax.tree.map(lambda a, b: jnp.where(reached, a, b), new, before)

    return lax.fori_loop(0, length, lap, start)


def passed_along(value, axis, steps):
    count = lax.axis_size(axis)
    first, last = (max(0, -steps), min(count, count - steps))
    return lax.ppermute(value, axis, [(source, source + steps) for source in range(first, last)])


def rotate(values, token_ordinal):
    half_dim = values.shape[-1] // 2
    frequency = 1.0 / ROPE_BASE ** jnp.linspace(0.0, 1.0, half_dim, dtype=jnp.float32)
    angles = token_ordinal[:, None] * frequency[None, :]
    cosine_table = jnp.cos(angles)[:, None, :]
    sine_table = jnp.sin(angles)[:, None, :]
    first = values[..., :half_dim].astype(jnp.float32)
    second = values[..., half_dim:].astype(jnp.float32)
    return jnp.concatenate(
        [first * cosine_table - second * sine_table, first * sine_table + second * cosine_table],
        axis=-1,
    )


def make_adder(normed, contracted, pieces):
    updated = []
    for member in range(len(pieces)):
        portion = pieces[member]
        if member < contracted:
            updated.append(jnp.dot(normed, portion, preferred_element_type=jnp.float32))
        else:
            updated.append(portion)
    return tuple(updated)


def retention_local(projections, decays, token_ordinal):
    tok_rows = token_ordinal.shape[0]
    head_count = decays.shape[0]
    blocks = tok_rows // BLOCK_LEN
    query_raw = projections[0].reshape(tok_rows, head_count, KEY_DIM)
    key_raw = projections[1].reshape(tok_rows, head_count, KEY_DIM)
    queries = rotate(query_raw, token_ordinal).astype(jnp.bfloat16)
    lookup_matrix_lines = (rotate(key_raw, token_ordinal) * KEY_DIM ** (-0.5)).astype(jnp.bfloat16)
    value_proj = projections[2].reshape(tok_rows, head_count, VALUE_DIM)

    def split_blocks(array):
        shaped = array.reshape(blocks, BLOCK_LEN, head_count, array.shape[-1])
        return jnp.transpose(shaped, (0, 2, 1, 3))

    query_blocks = split_blocks(queries)
    key_blocks = split_blocks(lookup_matrix_lines)
    value_blocks = split_blocks(value_proj)
    decay_blocks = jnp.transpose(decays.reshape(head_count, blocks, BLOCK_LEN), (1, 0, 2))
    cumulative = jnp.cumsum(decay_blocks, axis=-1)
    ending = cumulative[..., -1:]
    decay_gaps = cumulative[..., :, None] - cumulative[..., None, :]
    causal = jnp.arange(BLOCK_LEN)[:, None] >= jnp.arange(BLOCK_LEN)[None, :]
    weighting = jnp.where(causal, jnp.exp(jnp.minimum(decay_gaps, 0.0)), 0.0)
    raw_scores = jnp.einsum(
        "nhid,nhjd->nhij", query_blocks, key_blocks, preferred_element_type=jnp.float32
    )
    scores = (raw_scores * weighting).astype(jnp.bfloat16)
    intra_out = jnp.einsum(
        "nhij,nhje->nhie", scores, value_blocks, preferred_element_type=jnp.float32
    )
    decayed_keys = (
        key_blocks.astype(jnp.float32) * jnp.exp(ending - cumulative)[..., None]
    ).astype(jnp.bfloat16)
    decayed_queries = (query_blocks.astype(jnp.float32) * jnp.exp(cumulative)[..., None]).astype(
        jnp.bfloat16
    )
    block_kv = jnp.einsum(
        "nhjd,nhje->nhde", decayed_keys, value_blocks, preferred_element_type=jnp.float32
    )
    block_ends = ending[..., 0]

    def advance(state_now, step_in):
        kv_block, total = step_in
        return (state_now * jnp.exp(total)[:, None, None] + kv_block, state_now)

    start_state = jnp.zeros((head_count, KEY_DIM, VALUE_DIM), jnp.float32)
    end_state, before_local = lax.scan(advance, start_state, (block_kv, block_ends))
    device_total = jnp.sum(block_ends, axis=0)
    return (intra_out, decayed_queries, before_local, block_ends, end_state, device_total)


def combine(earlier, later):
    return (earlier[0] * jnp.exp(later[1])[:, None, None] + later[0], earlier[1] + later[1])


def carried(end_state, device_total):
    identity = (jnp.zeros_like(end_state), jnp.zeros_like(device_total))
    state_in, _ = entering((end_state, device_total), "sp", combine, identity)
    return state_in


def retention_finish(local_parts, state_in, gate_proj):
    intra_out, decayed_queries, before_local, block_ends, end_state, device_total = local_parts
    starts = jnp.cumsum(block_ends, axis=0) - block_ends
    full_states = before_local + jnp.exp(starts)[:, :, None, None] * state_in[None]
    cross = jnp.einsum(
        "nhid,nhde->nhie",
        decayed_queries,
        full_states.astype(jnp.bfloat16),
        preferred_element_type=jnp.float32,
    )
    output = intra_out + cross
    output = output * lax.rsqrt(jnp.mean(output * output, axis=-1, keepdims=True) + EPSILON)
    tok_rows = gate_proj.shape[0]
    output = jnp.transpose(output, (0, 2, 1, 3)).reshape(tok_rows, gate_proj.shape[1])
    return (output * jax.nn.silu(gate_proj.astype(jnp.float32))).astype(jnp.bfloat16)


def convolve(conv_proj, conv_kernel):
    gate_b, gate_c, conv_input = conv_proj
    tok_rows = gate_b.shape[0]
    product = gate_c.astype(jnp.float32) * conv_input.astype(jnp.float32)
    rim_rows = passed_along(product[tok_rows - (CONV_TAPS - 1) :], "sp", 1)
    padded = jnp.concatenate([rim_rows, product], axis=0)
    convolved = jnp.zeros_like(product)
    for tap_index in range(CONV_TAPS):
        convolved = convolved + conv_kernel[tap_index] * padded[tap_index : tap_index + tok_rows]
    return (gate_b.astype(jnp.float32) * convolved).astype(jnp.bfloat16)


def shards(
    tokens,
    norm_gain,
    query_weight,
    key_weight,
    value_weight,
    gate_weight,
    conv_b_weight,
    conv_c_weight,
    conv_in_weight,
    conv_kernel,
    out_ret_weight,
    out_conv_weight,
    log_decay,
):
    inputs = tokens[0].astype(jnp.float32)
    tok_rows = inputs.shape[0]
    normed = (
        inputs * lax.rsqrt(jnp.mean(inputs * inputs, axis=-1, keepdims=True) + EPSILON) * norm_gain
    ).astype(jnp.bfloat16)
    token_ordinal = (
        lax.axis_index("sp") * tok_rows + jnp.arange(tok_rows, dtype=jnp.int32)
    ).astype(jnp.float32)
    decays = log_decay[0]
    gathered = make_adder(
        normed,
        7,
        (
            lax.all_gather(query_weight, ("sp", "fs"), axis=0, tiled=True),
            lax.all_gather(key_weight, ("sp", "fs"), axis=0, tiled=True),
            lax.all_gather(value_weight, ("sp", "fs"), axis=0, tiled=True),
            lax.all_gather(gate_weight, ("sp", "fs"), axis=0, tiled=True),
            lax.all_gather(conv_b_weight, ("sp", "fs"), axis=0, tiled=True),
            lax.all_gather(conv_c_weight, ("sp", "fs"), axis=0, tiled=True),
            lax.all_gather(conv_in_weight, ("sp", "fs"), axis=0, tiled=True),
            lax.all_gather(out_ret_weight, ("sp", "fs"), axis=0, tiled=True),
            lax.all_gather(out_conv_weight, ("sp", "fs"), axis=0, tiled=True),
        ),
    )
    ret_proj = [member.astype(jnp.bfloat16) for member in gathered[:4]]
    local_parts = retention_local(ret_proj, decays, token_ordinal)
    state_in = carried(local_parts[4], local_parts[5])
    conv_proj = [member.astype(jnp.bfloat16) for member in gathered[4:7]]
    full_ret, full_conv = (gathered[7], gathered[8])
    conv_out = convolve(conv_proj, conv_kernel)
    ret_out = retention_finish(local_parts, state_in, ret_proj[3])
    partial_value = lax.dot_general(
        ret_out, full_ret, (((1,), (1,)), ((), ())), preferred_element_type=jnp.float32
    )
    mixed = lax.psum_scatter(
        (
            partial_value
            + lax.dot_general(
                conv_out, full_conv, (((1,), (1,)), ((), ())), preferred_element_type=jnp.float32
            )
        ).astype(jnp.bfloat16),
        "tp",
        scatter_dimension=0,
        tiled=True,
    )
    return mixed[None]


MESH_IDS = pl.DeviceIdType.MESH
OUT_CUT = 2
OUT_TILE = 512


def remote(source, target, sent, landed, device):
    return pltpu.make_async_remote_copy(
        src_ref=source,
        dst_ref=target,
        send_sem=sent,
        recv_sem=landed,
        device_id=device,
        device_id_type=MESH_IDS,
    )


def greet(peers):
    barrier = pltpu.get_barrier_semaphore()
    for peer in peers:
        pl.semaphore_signal(barrier, inc=1, device_id=peer, device_id_type=MESH_IDS)
    pl.semaphore_wait(barrier, len(peers))


def plane_partners(f):
    x, y = f % 2, f // 2
    return y * 2 + (1 - x), (1 - y) * 2 + x, 3 - f


def mixer_kernel(
    n_sp,
    tokens_ref,
    gain_ref,
    query_ref,
    key_ref,
    value_ref,
    gate_ref,
    conv_b_ref,
    conv_c_ref,
    conv_in_ref,
    taps_ref,
    out_ret_ref,
    out_conv_ref,
    decay_ref,
    near_cos_ref,
    near_sin_ref,
    base_ref,
    out_ref,
    raw_ref,
    normed_ref,
    pieces_ref,
    heads_ref,
    full_ref,
    outs_ref,
    decay_piece_ref,
    decays_ref,
    cos_ref,
    sin_ref,
    proj_ref,
    intra_ref,
    decayed_ref,
    before_ref,
    starts_ref,
    product_ref,
    state_ref,
    state_piece_ref,
    states_ref,
    extra_piece_ref,
    extras_ref,
    mixed_ref,
    merged_ref,
    part_ref,
    far_ref,
    local_sem,
    weight_sent,
    weight_landed,
    decay_sent,
    decay_landed,
    norm_sent,
    norm_landed,
    side_sent,
    side_landed,
    relay_sent,
    up_sent,
    down_sent,
    line_landed,
    wide_sent,
    wide_landed,
    wide_up_sent,
    wide_down_sent,
    wide_line_landed,
    slim_up_sent,
    slim_down_sent,
    slim_line_landed,
    slim_sent,
    slim_landed,
    slim_relay_sent,
    state_sent,
    state_landed,
    mixed_sent,
    mixed_landed,
    part_sent,
    part_landed,
):
    f32, bf16 = jnp.float32, jnp.bfloat16
    s, f, t = lax.axis_index("sp"), lax.axis_index("fs"), lax.axis_index("tp")
    xn, yn, dn = plane_partners(f)
    order = (xn, yn, dn)
    other = {"tp": 1 - t}
    n_fs, tok, model = normed_ref.shape
    half = tok // 2
    chunk = half // 2
    rows = query_ref.shape[0]
    blocks = tok // BLOCK_LEN
    lanes = 2 * KEY_DIM
    pair = 2 * VALUE_DIM
    halo = CONV_TAPS - 1
    cut = rows // OUT_CUT

    def lane(index, width):
        return pl.ds(pl.multiple_of(index * width, width), width)

    waits = []
    guarded = []

    def start(copy):
        copy.start()
        waits.append(copy)

    def start_when(condition, copy):
        @pl.when(condition)
        def _():
            copy.start()

        guarded.append((condition, copy))

    count = [0]

    def fetch(source, target):
        copy = pltpu.make_async_copy(source, target, local_sem.at[count[0]])
        count[0] += 1
        copy.start()
        return copy

    def block(b, g):
        return full_ref.at[pl.ds((b * n_fs + g) * rows, rows), :]

    def wide(b, g):
        return outs_ref.at[pl.ds((b * n_fs + g) * rows, cut), :]

    def slim(b, g):
        return outs_ref.at[pl.ds((b * n_fs + g) * rows + cut, rows - cut), :]

    head_loads = [fetch(query_ref, heads_ref.at[0]), fetch(key_ref, heads_ref.at[1])]
    wide_weights = (value_ref, gate_ref, conv_b_ref, conv_c_ref, conv_in_ref)
    piece_loads = []
    for p in range(n_fs):
        for j, weight in enumerate(wide_weights):
            piece_loads.append(
                fetch(
                    weight.at[:, pl.ds(p * VALUE_DIM, VALUE_DIM)],
                    pieces_ref.at[p, :, pl.ds(lanes + j * VALUE_DIM, VALUE_DIM)],
                )
            )
    own_loads = [
        fetch(
            weight.at[:, lane(f, VALUE_DIM)],
            full_ref.at[pl.ds((s * n_fs + f) * rows, rows), pl.ds(lanes + j * VALUE_DIM, VALUE_DIM)],
        )
        for j, weight in enumerate(wide_weights)
    ]
    raw_loads = [
        fetch(
            tokens_ref.at[0, pl.ds(t * half + i * chunk, chunk), :], raw_ref.at[pl.ds(i * chunk, chunk), :]
        )
        for i in range(2)
    ]
    out_loads = []
    for g in range(n_fs):
        for j, weight in enumerate((out_ret_ref, out_conv_ref)):
            out_loads.append(
                fetch(
                    weight.at[:, pl.ds(g * VALUE_DIM, VALUE_DIM)],
                    outs_ref.at[
                        pl.ds((s * n_fs + f) * rows, rows), pl.ds(g * pair + j * VALUE_DIM, VALUE_DIM)
                    ],
                )
            )
    table_loads = [fetch(near_cos_ref, cos_ref), fetch(near_sin_ref, sin_ref)]

    peers = [{"fs": p} for p in order] + [other]
    peers += [{"sp": (s + d) % n_sp} for d in range(1, n_sp)]
    greet(peers)

    for copy in head_loads:
        copy.wait()
    for p in range(n_fs):
        own = pl.ds(p * KEY_DIM, KEY_DIM)
        pieces_ref[p, :, 0:lanes] = jnp.concatenate([heads_ref[0, :, own], heads_ref[1, :, own]], axis=-1)
    full_ref[pl.ds((s * n_fs + f) * rows, rows), 0:lanes] = pieces_ref[f, :, 0:lanes]
    decay_piece_ref[...] = jnp.zeros_like(decay_piece_ref)
    for p in range(n_fs):
        for n in range(blocks):
            decay_piece_ref[p, n : n + 1, :] = decay_ref[0, p : p + 1, n * BLOCK_LEN : (n + 1) * BLOCK_LEN]
    decays_ref[f] = decay_piece_ref[f]
    for copy in piece_loads:
        copy.wait()
    for i, p in enumerate(order):
        start(remote(pieces_ref.at[p], block(s, f), weight_sent.at[i], weight_landed.at[f], {"fs": p}))

    def line(view, up, down, landed):
        def copy(source, way):
            return remote(source, view, up if way == 1 else down, landed, {"sp": s + way})

        def send():
            start_when(s < n_sp - 1, copy(view, 1))
            start_when(s > 0, copy(view, -1))

        def step(d, b, way, then):
            there = (s - d >= 0) if way == 1 else (s + d <= n_sp - 1)
            further = there & ((s < n_sp - 1) if way == 1 else (s > 0))

            @pl.when(there)
            def _():
                copy(view, way).wait_recv()

            start_when(further, copy(view, way))
            if then is not None:
                then(there)

        return send, step

    def weight_line(b, g):
        return line(block(b, g), up_sent.at[b, g], down_sent.at[b, g], line_landed.at[b, g])

    def wide_line(b, g):
        return line(wide(b, g), wide_up_sent.at[b, g], wide_down_sent.at[b, g], wide_line_landed.at[b, g])

    def slim_line(b):
        return line(slim(b, f), slim_up_sent.at[b], slim_down_sent.at[b], slim_line_landed.at[b])

    def walk(make, d, then=None):
        for way in (1, -1):
            b = s - way * d
            inside = (b >= 0) & (b <= n_sp - 1)
            b = jnp.where(inside, b, s)
            make(b)[1](d, b, way, None if then is None else (lambda there, b=b: then(there, b)))

    for copy in own_loads:
        copy.wait()
    weight_line(s, f)[0]()
    for i, p in enumerate(order):
        start(
            remote(decay_piece_ref.at[p], decays_ref.at[f], decay_sent.at[i], decay_landed.at[f], {"fs": p})
        )

    slab = 16

    def spot(owner, core, piece):
        return normed_ref.at[owner, pl.ds(core * half + piece * chunk, chunk), :]

    def normalise(piece):
        @pl.loop(0, chunk // slab)
        def _(i):
            x = raw_ref[pl.ds(piece * chunk + i * slab, slab), :].astype(f32)
            scale = lax.rsqrt(jnp.mean(x * x, axis=-1, keepdims=True) + EPSILON)
            normed_ref[f, pl.ds(t * half + piece * chunk + i * slab, slab), :] = (
                x * scale * gain_ref[...]
            ).astype(bf16)

    def norm_copy(piece, slot, p):
        return remote(
            spot(f, t, piece), spot(f, t, piece), norm_sent.at[slot], norm_landed.at[f, piece], {"fs": p}
        )

    def side_copy(owner, piece):
        view = spot(owner, t, piece)
        return remote(view, view, side_sent.at[owner, piece], side_landed.at[owner, piece], other)

    raw_loads[0].wait()
    normalise(0)
    start(norm_copy(0, 0, xn))
    raw_loads[1].wait()
    normalise(1)
    start(norm_copy(1, 1, yn))
    start(norm_copy(1, 2, xn))
    start(norm_copy(0, 3, yn))
    for piece in range(2):
        start(side_copy(f, piece))

    for p in order:
        remote(pieces_ref.at[p], block(s, p), weight_sent.at[0], weight_landed.at[p], {"fs": p}).wait_recv()
        weight_line(s, p)[0]()
    for copy in out_loads:
        copy.wait()
    for i, p in enumerate(order):
        start(remote(wide(s, f), wide(s, f), wide_sent.at[i], wide_landed.at[f], {"fs": p}))

    for copy in table_loads:
        copy.wait()

    @pl.loop(0, blocks)
    def _(n):
        at = pl.ds(n * BLOCK_LEN, BLOCK_LEN)
        near_cos, near_sin = cos_ref[at, :], sin_ref[at, :]
        cos_ref[at, :] = near_cos * base_ref[0, pl.ds(s, 1), :] - near_sin * base_ref[1, pl.ds(s, 1), :]
        sin_ref[at, :] = near_sin * base_ref[2, pl.ds(s, 1), :] + near_cos * base_ref[3, pl.ds(s, 1), :]

    for p in order:
        remote(
            decay_piece_ref.at[p], decays_ref.at[p], decay_sent.at[0], decay_landed.at[p], {"fs": p}
        ).wait_recv()
    for g in range(n_fs):
        total = decays_ref[g]
        places = lax.broadcasted_iota(jnp.int32, total.shape, 1)
        shift = 1
        while shift < BLOCK_LEN:
            total = total + jnp.where(places >= shift, pltpu.roll(total, shift, 1), 0.0)
            shift *= 2
        decays_ref[g] = total

    def arrived(owner, piece):
        view = spot(owner, t, piece)
        remote(view, view, norm_sent.at[0], norm_landed.at[owner, piece], {"fs": owner}).wait_recv()
        start(side_copy(owner, piece))

    def side_arrived(owner):
        for piece in range(2):
            view = spot(owner, 1 - t, piece)
            remote(view, view, side_sent.at[0, 0], side_landed.at[owner, piece], other).wait_recv()

    def weight_step(d):
        for g in (f,) + order:
            walk(lambda b, g=g: weight_line(b, g), d)

    weight_step(1)
    arrived(xn, 0)
    view = spot(xn, t, 0)
    start(remote(view, view, relay_sent.at[0], norm_landed.at[xn, 0], {"fs": yn}))
    arrived(yn, 1)
    view = spot(yn, t, 1)
    start(remote(view, view, relay_sent.at[1], norm_landed.at[yn, 1], {"fs": xn}))
    for d in range(2, n_sp - 1):
        weight_step(d)
    arrived(xn, 1)
    arrived(yn, 0)

    def slim_plane(b, i):
        return remote(
            slim(b, f), slim(b, f), slim_sent.at[b, i], slim_landed.at[b, f], {"fs": order[i]}
        )

    slim_line(s)[0]()
    for i in range(2):
        start(slim_plane(s, i))
    wide_line(s, f)[0]()
    for p in order:
        remote(wide(s, p), wide(s, p), wide_sent.at[0], wide_landed.at[p], {"fs": p}).wait_recv()
        wide_line(s, p)[0]()

    def slim_spread(there, b):
        for i in range(2):
            start_when(there, slim_plane(b, i))

    def out_step(d):
        walk(slim_line, d, slim_spread)
        for g in (f,) + order:
            walk(lambda b, g=g: wide_line(b, g), d)

    if n_sp > 2:
        weight_step(n_sp - 1)

    def project(o):
        @pl.loop(0, tok // chunk)
        def _(i):
            at = pl.ds(i * chunk, chunk)
            proj_ref[o, at, :] = jnp.dot(
                normed_ref[o, at, :], full_ref[...], preferred_element_type=f32
            ).astype(bf16)

    def part(o, at, index):
        return proj_ref[o, at, lanes + index * VALUE_DIM : lanes + (index + 1) * VALUE_DIM]

    causal = lax.broadcasted_iota(jnp.int32, (BLOCK_LEN, BLOCK_LEN), 0) >= lax.broadcasted_iota(
        jnp.int32, (BLOCK_LEN, BLOCK_LEN), 1
    )
    front = lax.broadcasted_iota(jnp.int32, (BLOCK_LEN, lanes), 1) % KEY_DIM < KEY_DIM // 2

    def retain(o):
        def body(n, carry):
            state, total = carry
            at = pl.ds(pl.multiple_of(n * BLOCK_LEN, BLOCK_LEN), BLOCK_LEN)
            row = decays_ref[o, pl.ds(n, 1), :]
            end = jnp.broadcast_to(row[:, BLOCK_LEN - 1 :], row.shape)
            across = jnp.broadcast_to(row, (BLOCK_LEN, BLOCK_LEN))
            down = across.T
            weighting = jnp.where(causal, jnp.exp(jnp.minimum(down - across, 0.0)), 0.0)
            x = proj_ref[o, at, 0:lanes].astype(f32)
            swapped = jnp.where(
                front, pltpu.roll(x, lanes - KEY_DIM // 2, 1), pltpu.roll(x, KEY_DIM // 2, 1)
            )
            turned = (x * cos_ref[at, :] + swapped * sin_ref[at, :]).astype(bf16)
            queries = turned[:, :KEY_DIM]
            keys = turned.astype(f32).T[KEY_DIM:, :]
            values = part(o, at, 0)
            raw = jnp.dot(queries, keys.astype(bf16), preferred_element_type=f32)
            scores = (raw * weighting).astype(bf16)
            intra_ref[o, at, :] = jnp.dot(scores, values, preferred_element_type=f32)
            decayed_ref[o, at, :] = (queries.astype(f32) * jnp.exp(down[:, :KEY_DIM])).astype(bf16)
            late = (keys * jnp.exp(end - row)).astype(bf16)
            before_ref[o, n] = state
            starts_ref[o, pl.ds(n, 1), :] = total
            product_ref[o, pl.ds(pl.multiple_of(8 + n * BLOCK_LEN, 8), BLOCK_LEN), :] = part(o, at, 3).astype(
                f32
            ) * part(o, at, 4).astype(f32)
            state = state * jnp.exp(end) + jnp.dot(late, values, preferred_element_type=f32)
            return state, total + end

        state, total = lax.fori_loop(
            0, blocks, body, (jnp.zeros((KEY_DIM, VALUE_DIM), f32), jnp.zeros((1, VALUE_DIM), f32))
        )
        state_piece_ref[o] = state.astype(bf16)
        extra_piece_ref[o] = jnp.broadcast_to(total, (8, VALUE_DIM))
        extra_piece_ref[o, 0:halo, :] = product_ref[o, 8 + tok - halo : 8 + tok, :]

    def state_copies(o, owner, d):
        return [
            remote(here, there, state_sent.at[o, d, k], state_landed.at[owner, o, k], {"sp": (s + d) % n_sp})
            for k, (here, there) in enumerate(
                (
                    (state_piece_ref.at[o], states_ref.at[owner, o]),
                    (extra_piece_ref.at[o], extras_ref.at[owner, o]),
                )
            )
        ]

    def pass_state(o):
        for d in range(1, n_sp):
            for copy in state_copies(o, s, d):
                start_when(s + d < n_sp, copy)

    def finish(o, put):
        state_ref[...] = jnp.zeros_like(state_ref)
        product_ref[o, 0:8, :] = jnp.zeros((8, VALUE_DIM), f32)
        for k in range(n_sp - 1):

            @pl.when(k < s)
            def _():
                for copy in state_copies(o, k, 1):
                    copy.wait_recv()
                state_ref[...] = state_ref[...] * jnp.exp(extras_ref[k, o, halo : halo + 1, :]) + states_ref[
                    k, o
                ].astype(f32)

            @pl.when(k == s - 1)
            def _():
                product_ref[o, 8 - halo : 8, :] = extras_ref[k, o, 0:halo, :]

        taps = [taps_ref[k : k + 1, lane(f, VALUE_DIM)] for k in range(CONV_TAPS)]

        @pl.loop(0, blocks)
        def _(n):
            at = pl.ds(pl.multiple_of(n * BLOCK_LEN, BLOCK_LEN), BLOCK_LEN)
            state = before_ref[o, n] + jnp.exp(starts_ref[o, pl.ds(n, 1), :]) * state_ref[...]
            output = intra_ref[o, at, :] + jnp.dot(
                decayed_ref[o, at, :], state.astype(bf16), preferred_element_type=f32
            )
            output = output * lax.rsqrt(jnp.mean(output * output, axis=-1, keepdims=True) + EPSILON)
            gate = part(o, at, 1).astype(f32)
            ret_out = (output * (gate / (1.0 + jnp.exp(-gate)))).astype(bf16)
            padded = product_ref[o, pl.ds(pl.multiple_of(n * BLOCK_LEN, 8), BLOCK_LEN + 8), :]
            convolved = sum(
                taps[k] * padded[8 - halo + k : 8 - halo + k + BLOCK_LEN, :] for k in range(CONV_TAPS)
            )
            conv_out = (part(o, at, 2).astype(f32) * convolved).astype(bf16)
            put(at, ret_out, conv_out)

    def send_mixed(o, i):
        def put(at, ret_out, conv_out):
            mixed_ref[i, at, 0:VALUE_DIM] = ret_out
            mixed_ref[i, at, VALUE_DIM:pair] = conv_out

        finish(o, put)
        start(
            remote(mixed_ref.at[i], merged_ref.at[:, lane(f, pair)], mixed_sent.at[i], mixed_landed.at[f], {"fs": o})
        )

    def keep(at, ret_out, conv_out):
        merged_ref[at, lane(2 * f, VALUE_DIM)] = ret_out
        merged_ref[at, lane(2 * f + 1, VALUE_DIM)] = conv_out

    def local_stage(o):
        side_arrived(o)
        project(o)
        retain(o)
        pass_state(o)

    local_stage(xn)
    local_stage(yn)
    send_mixed(xn, 0)
    arrived(dn, 0)
    arrived(dn, 1)
    local_stage(dn)
    send_mixed(yn, 1)
    out_step(1)

    def slim_arrived(b, g):
        remote(
            slim(b, g), slim(b, g), slim_relay_sent.at[0], slim_landed.at[b, g], {"fs": g}
        ).wait_recv()

    def slim_relay(b, first, onward):
        slim_arrived(b, first)
        start(
            remote(slim(b, first), slim(b, first), slim_relay_sent.at[b], slim_landed.at[b, first], {"fs": onward})
        )

    local_stage(f)
    send_mixed(dn, 2)
    for d in range(2, n_sp - 1):
        out_step(d)
    finish(f, keep)
    if n_sp > 2:
        out_step(n_sp - 1)
    for b in range(n_sp):
        first, onward = (xn, yn) if b < n_sp // 2 else (yn, xn)
        slim_relay(b, first, onward)
    for p in order:
        view = merged_ref.at[:, lane(p, pair)]
        remote(view, view, mixed_sent.at[0], mixed_landed.at[p], {"fs": p}).wait_recv()
    for b in range(n_sp):
        slim_arrived(b, yn if b < n_sp // 2 else xn)
        slim_arrived(b, dn)

    tiles = part_ref.shape[0]
    tile = part_ref.shape[2]

    def partial_tile(core, i):
        return lax.dot_general(
            merged_ref[pl.ds(core * half, half), :],
            outs_ref[pl.ds(pl.multiple_of(i * tile, tile), tile), :],
            (((1,), (1,)), ((), ())),
            preferred_element_type=f32,
        ).astype(bf16)

    def part_copy(i):
        return remote(part_ref.at[i], far_ref.at[i], part_sent.at[i], part_landed.at[i], other)

    @pl.loop(0, tiles)
    def _(i):
        part_ref[i] = partial_tile(1 - t, i)
        part_copy(i).start()

    @pl.loop(0, tiles)
    def _(i):
        mine = partial_tile(t, i).astype(f32)
        part_copy(i).wait_recv()
        out_ref[:, lane(i, tile)] = (mine + far_ref[i].astype(f32)).astype(bf16)

    @pl.loop(0, tiles)
    def _(i):
        part_copy(i).wait_send()

    for copy in waits:
        copy.wait_send()
    for condition, copy in guarded:

        @pl.when(condition)
        def _():
            copy.wait_send()


def fast_shards(
    tokens,
    norm_gain,
    query_weight,
    key_weight,
    value_weight,
    gate_weight,
    conv_b_weight,
    conv_c_weight,
    conv_in_weight,
    conv_kernel,
    out_ret_weight,
    out_conv_weight,
    log_decay,
):
    n_sp, n_fs = lax.axis_size("sp"), lax.axis_size("fs")
    tok, model = tokens.shape[1:]
    half = tok // 2
    blocks = tok // BLOCK_LEN
    rows = query_weight.shape[0]
    width = 2 * KEY_DIM + 5 * VALUE_DIM
    lanes, pair = 2 * KEY_DIM, 2 * VALUE_DIM
    tile = min(OUT_TILE, model)

    frequency = np.tile(1.0 / ROPE_BASE ** np.linspace(0.0, 1.0, KEY_DIM // 2), 4)
    near = np.arange(tok)[:, None] * frequency[None, :]
    far = (np.arange(n_sp) * tok)[:, None] * frequency[None, :]
    scale = np.where(np.arange(lanes) < KEY_DIM, 1.0, KEY_DIM ** (-0.5))
    sign = np.where(np.arange(lanes) % KEY_DIM < KEY_DIM // 2, -1.0, 1.0)
    base = np.stack(
        [np.cos(far) * scale, np.sin(far) * scale, np.cos(far) * scale * sign, np.sin(far) * scale * sign]
    )

    any_space = pl.BlockSpec(memory_space=pl.ANY)
    vmem = pl.BlockSpec(memory_space=pltpu.VMEM)
    dma = pltpu.SemaphoreType.DMA
    f32, bf16 = jnp.float32, jnp.bfloat16
    buffers = [
        ((half, model), bf16),
        ((n_fs, tok, model), bf16),
        ((n_fs, rows, width), bf16),
        ((2, rows, n_fs * KEY_DIM), bf16),
        ((n_sp * n_fs * rows, width), bf16),
        ((n_sp * n_fs * rows, n_fs * pair), bf16),
        ((n_fs, 8, BLOCK_LEN), f32),
        ((n_fs, 8, BLOCK_LEN), f32),
        ((tok, lanes), f32),
        ((tok, lanes), f32),
        ((n_fs, tok, width), bf16),
        ((n_fs, tok, VALUE_DIM), f32),
        ((n_fs, tok, KEY_DIM), bf16),
        ((n_fs, blocks, KEY_DIM, VALUE_DIM), f32),
        ((n_fs, 8, VALUE_DIM), f32),
        ((n_fs, 8 + tok, VALUE_DIM), f32),
        ((KEY_DIM, VALUE_DIM), f32),
        ((n_fs, KEY_DIM, VALUE_DIM), bf16),
        ((n_sp, n_fs, KEY_DIM, VALUE_DIM), bf16),
        ((n_fs, 8, VALUE_DIM), f32),
        ((n_sp, n_fs, 8, VALUE_DIM), f32),
        ((n_fs - 1, tok, pair), bf16),
        ((tok, n_fs * pair), bf16),
        ((model // tile, half, tile), bf16),
        ((model // tile, half, tile), bf16),
    ]
    semaphores = [
        (48,),
        (3,),
        (n_fs,),
        (3,),
        (n_fs,),
        (4,),
        (n_fs, 2),
        (n_fs, 2),
        (n_fs, 2),
        (2,),
        (n_sp, n_fs),
        (n_sp, n_fs),
        (n_sp, n_fs),
        (3,),
        (n_fs,),
        (n_sp, n_fs),
        (n_sp, n_fs),
        (n_sp, n_fs),
        (n_sp,),
        (n_sp,),
        (n_sp,),
        (n_sp, 2),
        (n_sp, n_fs),
        (n_sp,),
        (n_fs, n_sp, 2),
        (n_sp, n_fs, 2),
        (n_fs - 1,),
        (n_fs,),
        (model // tile,),
        (model // tile,),
    ]
    mixed = pl.pallas_call(
        lambda *refs: mixer_kernel(n_sp, *refs),
        out_shape=jax.ShapeDtypeStruct((half, model), bf16),
        in_specs=[any_space, vmem] + [any_space] * 7 + [vmem] + [any_space] * 2 + [vmem] + [any_space] * 2 + [vmem],
        out_specs=vmem,
        scratch_shapes=[pltpu.VMEM(shape, kind) for shape, kind in buffers] + [dma(shape) for shape in semaphores],
        compiler_params=pltpu.CompilerParams(
            collective_id=0, has_side_effects=True, vmem_limit_bytes=60 * 1024 * 1024
        ),
        name="mixer",
    )(
        tokens,
        norm_gain.reshape(1, model),
        query_weight,
        key_weight,
        value_weight,
        gate_weight,
        conv_b_weight,
        conv_c_weight,
        conv_in_weight,
        conv_kernel,
        out_ret_weight,
        out_conv_weight,
        log_decay,
        jnp.asarray(np.cos(near), jnp.float32),
        jnp.asarray(np.sin(near), jnp.float32),
        jnp.asarray(base, jnp.float32),
    )
    return mixed[None]


def select(mesh):
    def chosen(*arrays):
        heads, conv_width = arrays[12].shape[1], arrays[9].shape[1]
        n_sp, n_fs, n_tp = (mesh.shape[name] for name in ("sp", "fs", "tp"))
        tok, model = arrays[0].shape[1:]
        fits = n_fs == 4 and n_tp == 2 and n_sp > 2 and heads == n_fs
        fits = fits and conv_width == n_fs * VALUE_DIM and tok % (2 * BLOCK_LEN) == 0
        fits = fits and tok // BLOCK_LEN <= 8 and model % OUT_TILE == 0
        return (fast_shards if fits else shards)(*arrays)

    return chosen


def solution(mesh):
    in_specs = (
        P("fs", "sp", None),
        P(),
        P(("sp", "fs"), "tp"),
        P(("sp", "fs"), "tp"),
        P(("sp", "fs"), "tp"),
        P(("sp", "fs"), "tp"),
        P(("sp", "fs"), "tp"),
        P(("sp", "fs"), "tp"),
        P(("sp", "fs"), "tp"),
        P(None, "tp"),
        P(("sp", "fs"), "tp"),
        P(("sp", "fs"), "tp"),
        P("fs", "tp", "sp"),
    )
    out_specs = P("fs", ("sp", "tp"), None)
    return jax.shard_map(select(mesh), mesh=mesh, in_specs=in_specs, out_specs=out_specs, check_vma=False)
```

```python
import jax
import numpy as np
import jax.numpy as jnp
from jax import lax
from jax.experimental import pallas as pl
from jax.experimental.pallas import tpu as pltpu
from jax.sharding import PartitionSpec as P

KEY_DIM = 64
VALUE_DIM = 128
CONV_TAPS = 3
BLOCK_LEN = 128


EPSILON = 1e-06
ROPE_BASE = 10000.0


def entering(x, axis, combine, identity):
    length, here = (lax.axis_size(axis), lax.axis_index(axis))
    everything = jax.tree.map(
        lambda part, kind: lax.all_gather(part.astype(kind), axis), x, (jnp.bfloat16, jnp.bfloat16)
    )
    start = jax.tree.map(
        lambda part, zero: jnp.broadcast_to(jnp.asarray(zero, part.dtype), part.shape), x, identity
    )

    def lap(k, before):
        reached = k < here
        new = combine(
            before, jax.tree.map(lambda part, own: part[k].astype(own.dtype), everything, x)
        )
        return jax.tree.map(lambda a, b: jnp.where(reached, a, b), new, before)

    return lax.fori_loop(0, length, lap, start)


def passed_along(value, axis, steps):
    count = lax.axis_size(axis)
    first, last = (max(0, -steps), min(count, count - steps))
    return lax.ppermute(value, axis, [(source, source + steps) for source in range(first, last)])


def rotate(values, token_ordinal):
    half_dim = values.shape[-1] // 2
    frequency = 1.0 / ROPE_BASE ** jnp.linspace(0.0, 1.0, half_dim, dtype=jnp.float32)
    angles = token_ordinal[:, None] * frequency[None, :]
    cosine_table = jnp.cos(angles)[:, None, :]
    sine_table = jnp.sin(angles)[:, None, :]
    first = values[..., :half_dim].astype(jnp.float32)
    second = values[..., half_dim:].astype(jnp.float32)
    return jnp.concatenate(
        [first * cosine_table - second * sine_table, first * sine_table + second * cosine_table],
        axis=-1,
    )


def make_adder(normed, contracted, pieces):
    updated = []
    for member in range(len(pieces)):
        portion = pieces[member]
        if member < contracted:
            updated.append(jnp.dot(normed, portion, preferred_element_type=jnp.float32))
        else:
            updated.append(portion)
    return tuple(updated)


def retention_local(projections, decays, token_ordinal):
    tok_rows = token_ordinal.shape[0]
    head_count = decays.shape[0]
    blocks = tok_rows // BLOCK_LEN
    query_raw = projections[0].reshape(tok_rows, head_count, KEY_DIM)
    key_raw = projections[1].reshape(tok_rows, head_count, KEY_DIM)
    queries = rotate(query_raw, token_ordinal).astype(jnp.bfloat16)
    lookup_matrix_lines = (rotate(key_raw, token_ordinal) * KEY_DIM ** (-0.5)).astype(jnp.bfloat16)
    value_proj = projections[2].reshape(tok_rows, head_count, VALUE_DIM)

    def split_blocks(array):
        shaped = array.reshape(blocks, BLOCK_LEN, head_count, array.shape[-1])
        return jnp.transpose(shaped, (0, 2, 1, 3))

    query_blocks = split_blocks(queries)
    key_blocks = split_blocks(lookup_matrix_lines)
    value_blocks = split_blocks(value_proj)
    decay_blocks = jnp.transpose(decays.reshape(head_count, blocks, BLOCK_LEN), (1, 0, 2))
    cumulative = jnp.cumsum(decay_blocks, axis=-1)
    ending = cumulative[..., -1:]
    decay_gaps = cumulative[..., :, None] - cumulative[..., None, :]
    causal = jnp.arange(BLOCK_LEN)[:, None] >= jnp.arange(BLOCK_LEN)[None, :]
    weighting = jnp.where(causal, jnp.exp(jnp.minimum(decay_gaps, 0.0)), 0.0)
    raw_scores = jnp.einsum(
        "nhid,nhjd->nhij", query_blocks, key_blocks, preferred_element_type=jnp.float32
    )
    scores = (raw_scores * weighting).astype(jnp.bfloat16)
    intra_out = jnp.einsum(
        "nhij,nhje->nhie", scores, value_blocks, preferred_element_type=jnp.float32
    )
    decayed_keys = (
        key_blocks.astype(jnp.float32) * jnp.exp(ending - cumulative)[..., None]
    ).astype(jnp.bfloat16)
    decayed_queries = (query_blocks.astype(jnp.float32) * jnp.exp(cumulative)[..., None]).astype(
        jnp.bfloat16
    )
    block_kv = jnp.einsum(
        "nhjd,nhje->nhde", decayed_keys, value_blocks, preferred_element_type=jnp.float32
    )
    block_ends = ending[..., 0]

    def advance(state_now, step_in):
        kv_block, total = step_in
        return (state_now * jnp.exp(total)[:, None, None] + kv_block, state_now)

    start_state = jnp.zeros((head_count, KEY_DIM, VALUE_DIM), jnp.float32)
    end_state, before_local = lax.scan(advance, start_state, (block_kv, block_ends))
    device_total = jnp.sum(block_ends, axis=0)
    return (intra_out, decayed_queries, before_local, block_ends, end_state, device_total)


def combine(earlier, later):
    return (earlier[0] * jnp.exp(later[1])[:, None, None] + later[0], earlier[1] + later[1])


def carried(end_state, device_total):
    identity = (jnp.zeros_like(end_state), jnp.zeros_like(device_total))
    state_in, _ = entering((end_state, device_total), "sp", combine, identity)
    return state_in


def retention_finish(local_parts, state_in, gate_proj):
    intra_out, decayed_queries, before_local, block_ends, end_state, device_total = local_parts
    starts = jnp.cumsum(block_ends, axis=0) - block_ends
    full_states = before_local + jnp.exp(starts)[:, :, None, None] * state_in[None]
    cross = jnp.einsum(
        "nhid,nhde->nhie",
        decayed_queries,
        full_states.astype(jnp.bfloat16),
        preferred_element_type=jnp.float32,
    )
    output = intra_out + cross
    output = output * lax.rsqrt(jnp.mean(output * output, axis=-1, keepdims=True) + EPSILON)
    tok_rows = gate_proj.shape[0]
    output = jnp.transpose(output, (0, 2, 1, 3)).reshape(tok_rows, gate_proj.shape[1])
    return (output * jax.nn.silu(gate_proj.astype(jnp.float32))).astype(jnp.bfloat16)


def convolve(conv_proj, conv_kernel):
    gate_b, gate_c, conv_input = conv_proj
    tok_rows = gate_b.shape[0]
    product = gate_c.astype(jnp.float32) * conv_input.astype(jnp.float32)
    rim_rows = passed_along(product[tok_rows - (CONV_TAPS - 1) :], "sp", 1)
    padded = jnp.concatenate([rim_rows, product], axis=0)
    convolved = jnp.zeros_like(product)
    for tap_index in range(CONV_TAPS):
        convolved = convolved + conv_kernel[tap_index] * padded[tap_index : tap_index + tok_rows]
    return (gate_b.astype(jnp.float32) * convolved).astype(jnp.bfloat16)


def shards(
    tokens,
    norm_gain,
    query_weight,
    key_weight,
    value_weight,
    gate_weight,
    conv_b_weight,
    conv_c_weight,
    conv_in_weight,
    conv_kernel,
    out_ret_weight,
    out_conv_weight,
    log_decay,
):
    inputs = tokens[0].astype(jnp.float32)
    tok_rows = inputs.shape[0]
    normed = (
        inputs * lax.rsqrt(jnp.mean(inputs * inputs, axis=-1, keepdims=True) + EPSILON) * norm_gain
    ).astype(jnp.bfloat16)
    token_ordinal = (
        lax.axis_index("sp") * tok_rows + jnp.arange(tok_rows, dtype=jnp.int32)
    ).astype(jnp.float32)
    decays = log_decay[0]
    gathered = make_adder(
        normed,
        7,
        (
            lax.all_gather(query_weight, ("sp", "fs"), axis=0, tiled=True),
            lax.all_gather(key_weight, ("sp", "fs"), axis=0, tiled=True),
            lax.all_gather(value_weight, ("sp", "fs"), axis=0, tiled=True),
            lax.all_gather(gate_weight, ("sp", "fs"), axis=0, tiled=True),
            lax.all_gather(conv_b_weight, ("sp", "fs"), axis=0, tiled=True),
            lax.all_gather(conv_c_weight, ("sp", "fs"), axis=0, tiled=True),
            lax.all_gather(conv_in_weight, ("sp", "fs"), axis=0, tiled=True),
            lax.all_gather(out_ret_weight, ("sp", "fs"), axis=0, tiled=True),
            lax.all_gather(out_conv_weight, ("sp", "fs"), axis=0, tiled=True),
        ),
    )
    ret_proj = [member.astype(jnp.bfloat16) for member in gathered[:4]]
    local_parts = retention_local(ret_proj, decays, token_ordinal)
    state_in = carried(local_parts[4], local_parts[5])
    conv_proj = [member.astype(jnp.bfloat16) for member in gathered[4:7]]
    full_ret, full_conv = (gathered[7], gathered[8])
    conv_out = convolve(conv_proj, conv_kernel)
    ret_out = retention_finish(local_parts, state_in, ret_proj[3])
    partial_value = lax.dot_general(
        ret_out, full_ret, (((1,), (1,)), ((), ())), preferred_element_type=jnp.float32
    )
    mixed = lax.psum_scatter(
        (
            partial_value
            + lax.dot_general(
                conv_out, full_conv, (((1,), (1,)), ((), ())), preferred_element_type=jnp.float32
            )
        ).astype(jnp.bfloat16),
        "tp",
        scatter_dimension=0,
        tiled=True,
    )
    return mixed[None]


MESH_IDS = pl.DeviceIdType.MESH
WIDE_SHARE = 4


def remote(source, target, sent, landed, device):
    return pltpu.make_async_remote_copy(
        src_ref=source,
        dst_ref=target,
        send_sem=sent,
        recv_sem=landed,
        device_id=device,
        device_id_type=MESH_IDS,
    )


def greet(peers):
    barrier = pltpu.get_barrier_semaphore()
    for peer in peers:
        pl.semaphore_signal(barrier, inc=1, device_id=peer, device_id_type=MESH_IDS)
    pl.semaphore_wait(barrier, len(peers))


def plane_partners(f):
    x, y = f % 2, f // 2
    return y * 2 + (1 - x), (1 - y) * 2 + x, 3 - f


def mixer_kernel(
    n_sp,
    tokens_ref,
    gain_ref,
    query_ref,
    key_ref,
    value_ref,
    gate_ref,
    conv_b_ref,
    conv_c_ref,
    conv_in_ref,
    taps_ref,
    out_ret_ref,
    out_conv_ref,
    decay_ref,
    near_cos_ref,
    near_sin_ref,
    base_ref,
    out_ref,
    raw_ref,
    normed_ref,
    pieces_ref,
    heads_ref,
    full_ref,
    outs_ref,
    decay_piece_ref,
    decays_ref,
    cos_ref,
    sin_ref,
    early_ref,
    proj_ref,
    intra_ref,
    decayed_ref,
    before_ref,
    starts_ref,
    product_ref,
    state_ref,
    extra_ref,
    state_piece_ref,
    states_ref,
    mixed_ref,
    merged_ref,
    part_ref,
    far_ref,
    local_sem,
    send_sem,
    full_landed,
    wide_landed,
    slim_landed,
    norm_landed,
    side_landed,
    state_landed,
    part_landed,
    once_landed,
):
    f32, bf16 = jnp.float32, jnp.bfloat16
    scope = jax.named_scope
    s, f, t = lax.axis_index("sp"), lax.axis_index("fs"), lax.axis_index("tp")
    xn, yn, dn = plane_partners(f)
    order = (xn, yn, dn)
    other = {"tp": 1 - t}
    n_fs, tok, model = normed_ref.shape
    half = tok // 2
    chunk = half // 2
    rows = query_ref.shape[0]
    slab_rows = n_fs * rows
    blocks = tok // BLOCK_LEN
    lanes = 2 * KEY_DIM
    pair = 2 * VALUE_DIM
    halo = CONV_TAPS - 1
    cut = rows * WIDE_SHARE // 8

    def lane(index, width):
        return pl.ds(pl.multiple_of(index * width, width), width)

    names = (
        "weight", "decay", "norm", "side", "relay", "up", "down", "wide", "wide_relay", "wide_up", "wide_down",
        "slim", "slim_relay", "slim_up", "slim_down", "state", "mixed", "part",
    )
    sent = {name: send_sem.at[i] for i, name in enumerate(names)}

    def all_sent(name, view):
        remote(view, view, sent[name], once_landed.at[0], other).wait_send()

    def line_sent(name, view_of):
        for i in range(n_sp - 1):
            here = i if name.endswith("up") else n_sp - 1 - i

            @pl.when(s == here)
            def _(i=i):
                all_sent(name, view_of(i + 1))

    def fetch(source, target, slot):
        copy = pltpu.make_async_copy(source, target, local_sem.at[slot])
        copy.start()
        return copy

    def fetched(view, slot):
        pltpu.make_async_copy(view, view, local_sem.at[slot]).wait()

    def own_rows(b, g):
        return pl.ds((b * n_fs + g) * rows, rows)

    def block(b, g):
        return full_ref.at[own_rows(b, g), :]

    def wide(b, g):
        return outs_ref.at[pl.ds((b * n_fs + g) * rows, cut), :]

    def wide_half(g, i):
        width = outs_ref.shape[1] // 2
        return outs_ref.at[pl.ds((s * n_fs + g) * rows, cut), pl.ds(i * width, width)]

    def slim(b, g):
        return outs_ref.at[pl.ds((b * n_fs + g) * rows + cut, rows - cut), :]

    fetch(query_ref, heads_ref.at[0], 0)
    fetch(key_ref, heads_ref.at[1], 0)
    wide_weights = (value_ref, gate_ref, conv_b_ref, conv_c_ref, conv_in_ref)
    for p in range(n_fs):
        for j, weight in enumerate(wide_weights):
            fetch(
                weight.at[:, pl.ds(p * VALUE_DIM, VALUE_DIM)],
                pieces_ref.at[p, :, pl.ds(lanes + j * VALUE_DIM, VALUE_DIM)],
                1,
            )
    for j, weight in enumerate(wide_weights):
        fetch(
            weight.at[:, lane(f, VALUE_DIM)],
            full_ref.at[own_rows(s, f), pl.ds(lanes + j * VALUE_DIM, VALUE_DIM)],
            2,
        )
    for i in range(2):
        fetch(
            tokens_ref.at[0, pl.ds(t * half + i * chunk, chunk), :],
            raw_ref.at[pl.ds(i * chunk, chunk), :],
            3 + i,
        )
    for g in range(n_fs):
        for j, weight in enumerate((out_ret_ref, out_conv_ref)):
            fetch(
                weight.at[:, pl.ds(g * VALUE_DIM, VALUE_DIM)],
                outs_ref.at[own_rows(s, f), pl.ds(g * pair + j * VALUE_DIM, VALUE_DIM)],
                5,
            )
    tables = [fetch(near_cos_ref, cos_ref, 6), fetch(near_sin_ref, sin_ref, 7)]

    with scope("greet"):
        peers = [{"fs": p} for p in order] + [other]
        peers += [{"sp": (s + d) % n_sp} for d in range(1, n_sp)]
        greet(peers)

    fetched(heads_ref, 0)
    for p in range(n_fs):
        own = pl.ds(p * KEY_DIM, KEY_DIM)
        pieces_ref[p, :, 0:lanes] = jnp.concatenate([heads_ref[0, :, own], heads_ref[1, :, own]], axis=-1)
    full_ref[own_rows(s, f), 0:lanes] = pieces_ref[f, :, 0:lanes]
    decay_piece_ref[...] = jnp.zeros_like(decay_piece_ref)
    for p in range(n_fs):
        for n in range(blocks):
            decay_piece_ref[p, n : n + 1, :] = decay_ref[0, p : p + 1, n * BLOCK_LEN : (n + 1) * BLOCK_LEN]
    decays_ref[f] = decay_piece_ref[f]
    fetched(pieces_ref.at[:, :, lanes:], 1)
    for p in order:
        remote(pieces_ref.at[p], block(s, f), sent["weight"], full_landed.at[s, f], {"fs": p}).start()

    def line(view, up, down, landed):
        def copy(way):
            return remote(view, view, sent[up] if way == 1 else sent[down], landed, {"sp": s + way})

        def send():
            @pl.when(s < n_sp - 1)
            def _():
                copy(1).start()

            @pl.when(s > 0)
            def _():
                copy(-1).start()

        def step(way, there, then):
            further = (s < n_sp - 1) if way == 1 else (s > 0)

            @pl.when(there)
            def _():
                copy(way).wait_recv()

                @pl.when(further)
                def _():
                    copy(way).start()

                if then is not None:
                    then()

        return send, step

    def weight_line(b, g):
        return line(block(b, g), "up", "down", full_landed.at[b, g])

    def wide_line(b, g):
        return line(wide(b, g), "wide_up", "wide_down", wide_landed.at[b, g])

    def slim_line(b):
        return line(slim(b, f), "slim_up", "slim_down", slim_landed.at[b, f])

    def walk(make, d, then=None):
        for way in (1, -1):
            b = s - way * d
            there = (b >= 0) & (b <= n_sp - 1)
            b = jnp.where(there, b, s)
            make(b)[1](way, there, None if then is None else (lambda b=b: then(b)))

    fetched(full_ref.at[own_rows(s, f), lanes:], 2)
    weight_line(s, f)[0]()
    for p in order:
        remote(
            decay_piece_ref.at[p], decays_ref.at[f], sent["decay"], once_landed.at[1], {"fs": p}
        ).start()

    slab = 16

    def spot(owner, core, piece):
        return normed_ref.at[owner, pl.ds(core * half + piece * chunk, chunk), :]

    def normalise(piece):
        @pl.loop(0, chunk // slab)
        def _(i):
            x = raw_ref[pl.ds(piece * chunk + i * slab, slab), :].astype(f32)
            scale = lax.rsqrt(jnp.mean(x * x, axis=-1, keepdims=True) + EPSILON)
            normed_ref[f, pl.ds(t * half + piece * chunk + i * slab, slab), :] = (
                x * scale * gain_ref[...]
            ).astype(bf16)

    def norm_copy(owner, piece, kind, p):
        view = spot(owner, t, piece)
        return remote(view, view, sent[kind], norm_landed.at[owner, piece], {"fs": p})

    def side_copy(owner, piece):
        view = spot(owner, t, piece)
        remote(view, view, sent["side"], side_landed.at[owner], other).start()

    with scope("norm"):
        fetched(raw_ref.at[0:chunk, :], 3)
        normalise(0)
        norm_copy(f, 0, "norm", xn).start()
        fetched(raw_ref.at[chunk:half, :], 4)
        normalise(1)
        norm_copy(f, 1, "norm", yn).start()
        norm_copy(f, 1, "norm", xn).start()
        norm_copy(f, 0, "norm", yn).start()
        for piece in range(2):
            side_copy(f, piece)

    with scope("w_plane"):
        for p in order:
            remote(pieces_ref.at[p], block(s, p), sent["weight"], full_landed.at[s, p], {"fs": p}).wait_recv()
            weight_line(s, p)[0]()
    fetched(outs_ref.at[own_rows(s, f), :], 5)
    for p in order[:2]:
        remote(wide(s, f), wide(s, f), sent["wide"], wide_landed.at[s, f], {"fs": p}).start()

    for copy in tables:
        copy.wait()

    @pl.loop(0, blocks)
    def _(n):
        at = pl.ds(n * BLOCK_LEN, BLOCK_LEN)
        near_cos, near_sin = cos_ref[at, :], sin_ref[at, :]
        cos_ref[at, :] = near_cos * base_ref[0, pl.ds(s, 1), :] - near_sin * base_ref[1, pl.ds(s, 1), :]
        sin_ref[at, :] = near_sin * base_ref[2, pl.ds(s, 1), :] + near_cos * base_ref[3, pl.ds(s, 1), :]

    view = decay_piece_ref.at[0 : len(order)]
    remote(view, view, sent["decay"], once_landed.at[1], other).wait_recv()
    for g in range(n_fs):
        total = decays_ref[g]
        places = lax.broadcasted_iota(jnp.int32, total.shape, 1)
        shift = 1
        while shift < BLOCK_LEN:
            total = total + jnp.where(places >= shift, pltpu.roll(total, shift, 1), 0.0)
            shift *= 2
        decays_ref[g] = total

    def arrived(owner, piece):
        norm_copy(owner, piece, "norm", owner).wait_recv()
        side_copy(owner, piece)

    def side_arrived(owner):
        with scope("side"):
            view = normed_ref.at[owner, pl.ds((1 - t) * half, half), :]
            remote(view, view, sent["side"], side_landed.at[owner], other).wait_recv()

    def weight_step(d):
        with scope(f"w_line#d={d}"):
            for g in (f,) + order:
                walk(lambda b, g=g: weight_line(b, g), d)

    def nearest(k):
        ranked = [sorted(range(n_sp), key=lambda b: (abs(b - here), b))[k] for here in range(n_sp)]
        return sum(jnp.where(s == here, b, 0) for here, b in enumerate(ranked))

    def columns(o, at, b):
        return jnp.dot(
            normed_ref[o, at, lane(b, slab_rows)],
            full_ref[pl.ds(pl.multiple_of(b * slab_rows, slab_rows), slab_rows), :],
            preferred_element_type=f32,
        )

    def project_early(o, i):
        side_arrived(o)
        with scope("early"):
            near = [nearest(k) for k in range(n_sp - 1)]

            @pl.loop(0, tok // chunk)
            def _(j):
                at = pl.ds(j * chunk, chunk)
                early_ref[i, at, :] = sum(columns(o, at, b) for b in near)

    def project_late(o, i):
        with scope("late"):
            last = nearest(n_sp - 1)

            @pl.loop(0, tok // chunk)
            def _(j):
                at = pl.ds(j * chunk, chunk)
                proj_ref[o, at, :] = (early_ref[i, at, :] + columns(o, at, last)).astype(bf16)

    def project(o):
        side_arrived(o)
        with scope("project"):

            @pl.loop(0, tok // chunk)
            def _(j):
                at = pl.ds(j * chunk, chunk)
                proj_ref[o, at, :] = jnp.dot(
                    normed_ref[o, at, :], full_ref[...], preferred_element_type=f32
                ).astype(bf16)

    weight_step(1)
    with scope("x_first"):
        arrived(xn, 0)
        norm_copy(xn, 0, "relay", yn).start()
        arrived(yn, 1)
        norm_copy(yn, 1, "relay", xn).start()
    for d in range(2, n_sp - 1):
        weight_step(d)
    slim_line(s)[0]()
    wide_line(s, f)[0]()
    project_early(f, 0)
    with scope("x_second"):
        arrived(xn, 1)
        arrived(yn, 0)

    with scope("wide_plane"):
        for i, p in enumerate(order[:2]):
            remote(wide(s, p), wide(s, p), sent["wide"], wide_landed.at[s, p], {"fs": p}).wait_recv()
            view = wide_half(p, i)
            remote(view, view, sent["wide_relay"], wide_landed.at[s, p], {"fs": order[1 - i]}).start()

    def wide_far():
        with scope("wide_far"):
            remote(wide(s, dn), wide(s, dn), sent["wide"], wide_landed.at[s, dn], {"fs": dn}).wait_recv()

    def slim_spread(b):
        for p in order[:2]:
            remote(slim(b, f), slim(b, f), sent["slim"], slim_landed.at[b, f], {"fs": p}).start()

    def slim_arrived(b, g):
        remote(slim(b, g), slim(b, g), sent["slim"], slim_landed.at[b, g], {"fs": g}).wait_recv()

    def at_distance(d):
        for way in (1, -1) if d else (1,):
            b = s - way * d
            there = (b >= 0) & (b <= n_sp - 1)
            yield jnp.where(there, b, s), there

    def slim_plane(d):
        for b, there in at_distance(d):
            pl.when(there)(lambda b=b: slim_spread(b))

    def slim_relay(d):
        with scope(f"relay#d={d}"):
            for b, there in at_distance(d):
                near = b < n_sp // 2
                first, onward = jnp.where(near, xn, yn), jnp.where(near, yn, xn)

                @pl.when(there)
                def _():
                    slim_arrived(b, first)
                    view = slim(b, first)
                    remote(view, view, sent["slim_relay"], slim_landed.at[b, first], {"fs": onward}).start()

    def slim_rest(d):
        for b, there in at_distance(d):

            @pl.when(there)
            def _():
                slim_arrived(b, jnp.where(b < n_sp // 2, yn, xn))
                slim_arrived(b, dn)

    def slim_step(d):
        with scope(f"slim#d={d}"):
            walk(slim_line, d)

    def wide_step(d, g):
        with scope(f"wide#d={d}"):
            walk(lambda b: wide_line(b, g), d)

    def part(o, at, index):
        return proj_ref[o, at, lanes + index * VALUE_DIM : lanes + (index + 1) * VALUE_DIM]

    causal = lax.broadcasted_iota(jnp.int32, (BLOCK_LEN, BLOCK_LEN), 0) >= lax.broadcasted_iota(
        jnp.int32, (BLOCK_LEN, BLOCK_LEN), 1
    )
    front = lax.broadcasted_iota(jnp.int32, (BLOCK_LEN, lanes), 1) % KEY_DIM < KEY_DIM // 2

    def rounded(x):
        return x.astype(bf16).astype(f32)

    def retain(o):
        def body(n, carry):
            state, total = carry
            at = pl.ds(pl.multiple_of(n * BLOCK_LEN, BLOCK_LEN), BLOCK_LEN)
            row = decays_ref[o, pl.ds(n, 1), :]
            end = jnp.broadcast_to(row[:, BLOCK_LEN - 1 :], row.shape)
            across = jnp.broadcast_to(row, (BLOCK_LEN, BLOCK_LEN))
            down = across.T
            weighting = jnp.where(causal, jnp.exp(jnp.minimum(down - across, 0.0)), 0.0)
            x = proj_ref[o, at, 0:lanes].astype(f32)
            swapped = jnp.where(
                front, pltpu.roll(x, lanes - KEY_DIM // 2, 1), pltpu.roll(x, KEY_DIM // 2, 1)
            )
            turned = (x * cos_ref[at, :] + swapped * sin_ref[at, :]).astype(bf16)
            queries = turned[:, :KEY_DIM]
            keys = turned.astype(f32).T[KEY_DIM:, :]
            values = part(o, at, 0)
            raw = jnp.dot(queries, keys.astype(bf16), preferred_element_type=f32)
            scores = (raw * weighting).astype(bf16)
            intra_ref[o, at, :] = jnp.dot(scores, values, preferred_element_type=f32)
            decayed_ref[o, at, :] = (queries.astype(f32) * jnp.exp(down[:, :KEY_DIM])).astype(bf16)
            late = (keys * jnp.exp(end - row)).astype(bf16)
            before_ref[o, n] = state
            starts_ref[o, pl.ds(n, 1), :] = total
            product_ref[o, pl.ds(pl.multiple_of(8 + n * BLOCK_LEN, 8), BLOCK_LEN), :] = part(o, at, 3).astype(
                f32
            ) * part(o, at, 4).astype(f32)
            state = state * jnp.exp(end) + jnp.dot(late, values, preferred_element_type=f32)
            return state, total + end

        with scope("retain"):
            state, total = lax.fori_loop(
                0, blocks, body, (jnp.zeros((KEY_DIM, VALUE_DIM), f32), jnp.zeros((1, VALUE_DIM), f32))
            )
            rim = product_ref[o, 8 + tok - halo : 8 + tok, :]
            middle = total - rounded(total)
            extra_ref[...] = jnp.zeros_like(extra_ref)
            extra_ref[0:halo, :] = rounded(rim)
            extra_ref[halo : 2 * halo, :] = rim - rounded(rim)
            extra_ref[8:9, :] = rounded(total)
            extra_ref[9:10, :] = rounded(middle)
            extra_ref[10:11, :] = middle - rounded(middle)
            state_piece_ref[o, 0:KEY_DIM, :] = state.astype(bf16)
            state_piece_ref[o, KEY_DIM:, :] = extra_ref[...].astype(bf16)
            for d in range(1, n_sp):

                @pl.when(s + d < n_sp)
                def _():
                    state_copy(o, s, d).start()

    def state_copy(o, owner, d):
        return remote(
            state_piece_ref.at[o],
            states_ref.at[owner, o],
            sent["state"],
            state_landed.at[owner, o],
            {"sp": (s + d) % n_sp},
        )

    def finish(o, put):
        with scope("state"):
            state_ref[...] = jnp.zeros_like(state_ref)
            product_ref[o, 0:8, :] = jnp.zeros((8, VALUE_DIM), f32)
            for k in range(n_sp - 1):

                @pl.when(k < s)
                def _():
                    state_copy(o, k, 1).wait_recv()
                    extra_ref[...] = states_ref[k, o, KEY_DIM:, :].astype(f32)
                    total = extra_ref[8:9, :] + extra_ref[9:10, :] + extra_ref[10:11, :]
                    state_ref[...] = state_ref[...] * jnp.exp(total) + states_ref[k, o, 0:KEY_DIM, :].astype(f32)

                @pl.when(k == s - 1)
                def _():
                    product_ref[o, 8 - halo : 8, :] = extra_ref[0:halo, :] + extra_ref[halo : 2 * halo, :]

        taps = [taps_ref[k : k + 1, lane(f, VALUE_DIM)] for k in range(CONV_TAPS)]
        with scope("finish"):

            @pl.loop(0, blocks)
            def _(n):
                at = pl.ds(pl.multiple_of(n * BLOCK_LEN, BLOCK_LEN), BLOCK_LEN)
                state = before_ref[o, n] + jnp.exp(starts_ref[o, pl.ds(n, 1), :]) * state_ref[...]
                output = intra_ref[o, at, :] + jnp.dot(
                    decayed_ref[o, at, :], state.astype(bf16), preferred_element_type=f32
                )
                output = output * lax.rsqrt(jnp.mean(output * output, axis=-1, keepdims=True) + EPSILON)
                gate = part(o, at, 1).astype(f32)
                ret_out = (output * (gate / (1.0 + jnp.exp(-gate)))).astype(bf16)
                padded = product_ref[o, pl.ds(pl.multiple_of(n * BLOCK_LEN, 8), BLOCK_LEN + 8), :]
                convolved = sum(
                    taps[k] * padded[8 - halo + k : 8 - halo + k + BLOCK_LEN, :] for k in range(CONV_TAPS)
                )
                conv_out = (part(o, at, 2).astype(f32) * convolved).astype(bf16)
                put(at, ret_out, conv_out)

    def mixed_out(o, i):
        def put(at, ret_out, conv_out):
            mixed_ref[i, at, 0:VALUE_DIM] = ret_out
            mixed_ref[i, at, VALUE_DIM:pair] = conv_out

        finish(o, put)
        remote(
            mixed_ref.at[i], merged_ref.at[:, lane(f, pair)], sent["mixed"], once_landed.at[2], {"fs": o}
        ).start()

    def keep(at, ret_out, conv_out):
        merged_ref[at, lane(2 * f, VALUE_DIM)] = ret_out
        merged_ref[at, lane(2 * f + 1, VALUE_DIM)] = conv_out

    middle = range(2, n_sp - 1)
    project_early(xn, 1)
    project_early(yn, 2)
    weight_step(n_sp - 1)
    project_late(xn, 1)
    retain(xn)
    slim_step(1)
    wide_line(s, xn)[0]()
    project_late(yn, 2)
    retain(yn)
    for d in middle:
        slim_step(d)
    wide_step(1, f)
    mixed_out(xn, 0)
    mixed_out(yn, 1)
    wide_step(1, xn)
    with scope("x_third"):
        arrived(dn, 0)
        arrived(dn, 1)
    for d in range(n_sp - 1):
        slim_plane(d)
    project(dn)
    slim_step(n_sp - 1)
    retain(dn)
    wide_far()
    wide_line(s, yn)[0]()
    wide_line(s, dn)[0]()
    project_late(f, 0)
    for d in middle:
        wide_step(d, f)
    mixed_out(dn, 2)
    slim_plane(n_sp - 1)
    for d in middle:
        wide_step(d, xn)
    retain(f)
    slim_relay(0)
    wide_step(1, yn)
    finish(f, keep)
    wide_step(1, dn)
    slim_relay(1)
    for d in middle:
        wide_step(d, yn)
        wide_step(d, dn)
    for d in range(2, n_sp):
        slim_relay(d)
    with scope("settle"):
        all_sent("weight", pieces_ref.at[0 : len(order)])
        all_sent("decay", decay_piece_ref.at[0 : len(order)])
        all_sent("norm", normed_ref.at[0])
        all_sent("relay", normed_ref.at[0, 0:half, :])
        all_sent("side", normed_ref.at[0:2])
        all_sent("wide", outs_ref.at[0 : 2 * cut, :])
        all_sent("wide_relay", outs_ref.at[0:cut, :])
        for way in ("up", "down"):
            line_sent(way, lambda k: full_ref.at[0 : k * slab_rows, :])
            line_sent("slim_" + way, lambda k: outs_ref.at[0 : k * (rows - cut), :])
        for k in range(1, n_sp):

            @pl.when(s == n_sp - 1 - k)
            def _(k=k):
                all_sent("state", states_ref.at[0:k])

    with scope("h_wait"):
        view = merged_ref.at[:, 0 : len(order) * pair]
        remote(view, view, sent["mixed"], once_landed.at[2], other).wait_recv()

    def part_copy(b):
        return remote(part_ref.at[0, b], far_ref.at[b], sent["part"], part_landed.at[b], other)

    def out_tile(b):
        @pl.loop(0, 2)
        def _(j):
            core = jnp.where(j == 0, 1 - t, t)
            part_ref[j, b] = lax.dot_general(
                merged_ref[pl.ds(pl.multiple_of(core * half, half), half), :],
                outs_ref[pl.ds(pl.multiple_of(b * slab_rows, slab_rows), slab_rows), :],
                (((1,), (1,)), ((), ())),
                preferred_element_type=f32,
            ).astype(bf16)

            @pl.when(j == 0)
            def _():
                part_copy(b).start()

    def out_sum(k):
        with scope("o_sum"):
            b = nearest(k)
            part_copy(b).wait_recv()
            out_ref[:, lane(b, slab_rows)] = (part_ref[1, b].astype(f32) + far_ref[b].astype(f32)).astype(bf16)

    for k in range(n_sp):
        with scope(f"o_wait#k={k}"):
            if k == n_sp - 1:
                for g in (f,) + order:
                    wide_step(k, g)
            slim_rest(k)
        with scope(f"o_tile#k={k}"):
            out_tile(nearest(k))
        if k > 0:
            out_sum(k - 1)
    with scope("o_settle"):
        for way in ("up", "down"):
            line_sent("wide_" + way, lambda k: outs_ref.at[0 : k * n_fs * cut, :])
        all_sent("slim", outs_ref.at[0 : 2 * n_sp * (rows - cut), :])
        all_sent("slim_relay", outs_ref.at[0 : n_sp * (rows - cut), :])
        all_sent("mixed", mixed_ref)
        all_sent("part", far_ref)
    out_sum(n_sp - 1)


def fast_shards(
    tokens,
    norm_gain,
    query_weight,
    key_weight,
    value_weight,
    gate_weight,
    conv_b_weight,
    conv_c_weight,
    conv_in_weight,
    conv_kernel,
    out_ret_weight,
    out_conv_weight,
    log_decay,
):
    n_sp, n_fs = lax.axis_size("sp"), lax.axis_size("fs")
    tok, model = tokens.shape[1:]
    half = tok // 2
    blocks = tok // BLOCK_LEN
    rows = query_weight.shape[0]
    width = 2 * KEY_DIM + 5 * VALUE_DIM
    lanes, pair = 2 * KEY_DIM, 2 * VALUE_DIM

    frequency = np.tile(1.0 / ROPE_BASE ** np.linspace(0.0, 1.0, KEY_DIM // 2), 4)
    near = np.arange(tok)[:, None] * frequency[None, :]
    far = (np.arange(n_sp) * tok)[:, None] * frequency[None, :]
    scale = np.where(np.arange(lanes) < KEY_DIM, 1.0, KEY_DIM ** (-0.5))
    sign = np.where(np.arange(lanes) % KEY_DIM < KEY_DIM // 2, -1.0, 1.0)
    base = np.stack(
        [np.cos(far) * scale, np.sin(far) * scale, np.cos(far) * scale * sign, np.sin(far) * scale * sign]
    )

    any_space = pl.BlockSpec(memory_space=pl.ANY)
    vmem = pl.BlockSpec(memory_space=pltpu.VMEM)
    dma = pltpu.SemaphoreType.DMA
    f32, bf16 = jnp.float32, jnp.bfloat16
    buffers = [
        ((half, model), bf16),
        ((n_fs, tok, model), bf16),
        ((n_fs, rows, width), bf16),
        ((2, rows, n_fs * KEY_DIM), bf16),
        ((n_sp * n_fs * rows, width), bf16),
        ((n_sp * n_fs * rows, n_fs * pair), bf16),
        ((n_fs, 8, BLOCK_LEN), f32),
        ((n_fs, 8, BLOCK_LEN), f32),
        ((tok, lanes), f32),
        ((tok, lanes), f32),
        ((n_fs - 1, tok, width), f32),
        ((n_fs, tok, width), bf16),
        ((n_fs, tok, VALUE_DIM), f32),
        ((n_fs, tok, KEY_DIM), bf16),
        ((n_fs, blocks, KEY_DIM, VALUE_DIM), f32),
        ((n_fs, 8, VALUE_DIM), f32),
        ((n_fs, 8 + tok, VALUE_DIM), f32),
        ((KEY_DIM, VALUE_DIM), f32),
        ((16, VALUE_DIM), f32),
        ((n_fs, KEY_DIM + 16, VALUE_DIM), bf16),
        ((n_sp, n_fs, KEY_DIM + 16, VALUE_DIM), bf16),
        ((n_fs - 1, tok, pair), bf16),
        ((tok, n_fs * pair), bf16),
        ((2, n_sp, half, n_fs * rows), bf16),
        ((n_sp, half, n_fs * rows), bf16),
    ]
    semaphores = [
        (8,),
        (18,),
        (n_sp, n_fs),
        (n_sp, n_fs),
        (n_sp, n_fs),
        (n_fs, 2),
        (n_fs,),
        (n_sp, n_fs),
        (n_sp,),
        (3,),
    ]
    mixed = pl.pallas_call(
        lambda *refs: mixer_kernel(n_sp, *refs),
        out_shape=jax.ShapeDtypeStruct((half, model), bf16),
        in_specs=[any_space, vmem] + [any_space] * 7 + [vmem] + [any_space] * 2 + [vmem] + [any_space] * 2 + [vmem],
        out_specs=vmem,
        scratch_shapes=[pltpu.VMEM(shape, kind) for shape, kind in buffers] + [dma(shape) for shape in semaphores],
        compiler_params=pltpu.CompilerParams(
            collective_id=0, has_side_effects=True, vmem_limit_bytes=60 * 1024 * 1024
        ),
        name="mixer",
    )(
        tokens,
        norm_gain.reshape(1, model),
        query_weight,
        key_weight,
        value_weight,
        gate_weight,
        conv_b_weight,
        conv_c_weight,
        conv_in_weight,
        conv_kernel,
        out_ret_weight,
        out_conv_weight,
        log_decay,
        jnp.asarray(np.cos(near), jnp.float32),
        jnp.asarray(np.sin(near), jnp.float32),
        jnp.asarray(base, jnp.float32),
    )
    return mixed[None]


def select(mesh):
    def chosen(*arrays):
        heads, conv_width = arrays[12].shape[1], arrays[9].shape[1]
        n_sp, n_fs, n_tp = (mesh.shape[name] for name in ("sp", "fs", "tp"))
        tok, model = arrays[0].shape[1:]
        fits = n_fs == 4 and n_tp == 2 and n_sp > 2 and heads == n_fs
        fits = fits and conv_width == n_fs * VALUE_DIM and tok % (2 * BLOCK_LEN) == 0
        fits = fits and tok // BLOCK_LEN <= 8 and arrays[10].shape[0] % BLOCK_LEN == 0
        return (fast_shards if fits else shards)(*arrays)

    return chosen


def solution(mesh):
    in_specs = (
        P("fs", "sp", None),
        P(),
        P(("sp", "fs"), "tp"),
        P(("sp", "fs"), "tp"),
        P(("sp", "fs"), "tp"),
        P(("sp", "fs"), "tp"),
        P(("sp", "fs"), "tp"),
        P(("sp", "fs"), "tp"),
        P(("sp", "fs"), "tp"),
        P(None, "tp"),
        P(("sp", "fs"), "tp"),
        P(("sp", "fs"), "tp"),
        P("fs", "tp", "sp"),
    )
    out_specs = P("fs", ("sp", "tp"), None)
    return jax.shard_map(select(mesh), mesh=mesh, in_specs=in_specs, out_specs=out_specs, check_vma=False)
```

```python
import jax
import numpy as np
import jax.numpy as jnp
from jax import lax
from jax.experimental import pallas as pl
from jax.experimental.pallas import tpu as pltpu
from jax.sharding import PartitionSpec as P

KEY_DIM = 64
VALUE_DIM = 128
CONV_TAPS = 3
BLOCK_LEN = 128


EPSILON = 1e-06
ROPE_BASE = 10000.0


def entering(x, axis, combine, identity):
    length, here = (lax.axis_size(axis), lax.axis_index(axis))
    everything = jax.tree.map(
        lambda part, kind: lax.all_gather(part.astype(kind), axis), x, (jnp.bfloat16, jnp.bfloat16)
    )
    start = jax.tree.map(
        lambda part, zero: jnp.broadcast_to(jnp.asarray(zero, part.dtype), part.shape), x, identity
    )

    def lap(k, before):
        reached = k < here
        new = combine(
            before, jax.tree.map(lambda part, own: part[k].astype(own.dtype), everything, x)
        )
        return jax.tree.map(lambda a, b: jnp.where(reached, a, b), new, before)

    return lax.fori_loop(0, length, lap, start)


def passed_along(value, axis, steps):
    count = lax.axis_size(axis)
    first, last = (max(0, -steps), min(count, count - steps))
    return lax.ppermute(value, axis, [(source, source + steps) for source in range(first, last)])


def rotate(values, token_ordinal):
    half_dim = values.shape[-1] // 2
    frequency = 1.0 / ROPE_BASE ** jnp.linspace(0.0, 1.0, half_dim, dtype=jnp.float32)
    angles = token_ordinal[:, None] * frequency[None, :]
    cosine_table = jnp.cos(angles)[:, None, :]
    sine_table = jnp.sin(angles)[:, None, :]
    first = values[..., :half_dim].astype(jnp.float32)
    second = values[..., half_dim:].astype(jnp.float32)
    return jnp.concatenate(
        [first * cosine_table - second * sine_table, first * sine_table + second * cosine_table],
        axis=-1,
    )


def make_adder(normed, contracted, pieces):
    updated = []
    for member in range(len(pieces)):
        portion = pieces[member]
        if member < contracted:
            updated.append(jnp.dot(normed, portion, preferred_element_type=jnp.float32))
        else:
            updated.append(portion)
    return tuple(updated)


def retention_local(projections, decays, token_ordinal):
    tok_rows = token_ordinal.shape[0]
    head_count = decays.shape[0]
    blocks = tok_rows // BLOCK_LEN
    query_raw = projections[0].reshape(tok_rows, head_count, KEY_DIM)
    key_raw = projections[1].reshape(tok_rows, head_count, KEY_DIM)
    queries = rotate(query_raw, token_ordinal).astype(jnp.bfloat16)
    lookup_matrix_lines = (rotate(key_raw, token_ordinal) * KEY_DIM ** (-0.5)).astype(jnp.bfloat16)
    value_proj = projections[2].reshape(tok_rows, head_count, VALUE_DIM)

    def split_blocks(array):
        shaped = array.reshape(blocks, BLOCK_LEN, head_count, array.shape[-1])
        return jnp.transpose(shaped, (0, 2, 1, 3))

    query_blocks = split_blocks(queries)
    key_blocks = split_blocks(lookup_matrix_lines)
    value_blocks = split_blocks(value_proj)
    decay_blocks = jnp.transpose(decays.reshape(head_count, blocks, BLOCK_LEN), (1, 0, 2))
    cumulative = jnp.cumsum(decay_blocks, axis=-1)
    ending = cumulative[..., -1:]
    decay_gaps = cumulative[..., :, None] - cumulative[..., None, :]
    causal = jnp.arange(BLOCK_LEN)[:, None] >= jnp.arange(BLOCK_LEN)[None, :]
    weighting = jnp.where(causal, jnp.exp(jnp.minimum(decay_gaps, 0.0)), 0.0)
    raw_scores = jnp.einsum(
        "nhid,nhjd->nhij", query_blocks, key_blocks, preferred_element_type=jnp.float32
    )
    scores = (raw_scores * weighting).astype(jnp.bfloat16)
    intra_out = jnp.einsum(
        "nhij,nhje->nhie", scores, value_blocks, preferred_element_type=jnp.float32
    )
    decayed_keys = (
        key_blocks.astype(jnp.float32) * jnp.exp(ending - cumulative)[..., None]
    ).astype(jnp.bfloat16)
    decayed_queries = (query_blocks.astype(jnp.float32) * jnp.exp(cumulative)[..., None]).astype(
        jnp.bfloat16
    )
    block_kv = jnp.einsum(
        "nhjd,nhje->nhde", decayed_keys, value_blocks, preferred_element_type=jnp.float32
    )
    block_ends = ending[..., 0]

    def advance(state_now, step_in):
        kv_block, total = step_in
        return (state_now * jnp.exp(total)[:, None, None] + kv_block, state_now)

    start_state = jnp.zeros((head_count, KEY_DIM, VALUE_DIM), jnp.float32)
    end_state, before_local = lax.scan(advance, start_state, (block_kv, block_ends))
    device_total = jnp.sum(block_ends, axis=0)
    return (intra_out, decayed_queries, before_local, block_ends, end_state, device_total)


def combine(earlier, later):
    return (earlier[0] * jnp.exp(later[1])[:, None, None] + later[0], earlier[1] + later[1])


def carried(end_state, device_total):
    identity = (jnp.zeros_like(end_state), jnp.zeros_like(device_total))
    state_in, _ = entering((end_state, device_total), "sp", combine, identity)
    return state_in


def retention_finish(local_parts, state_in, gate_proj):
    intra_out, decayed_queries, before_local, block_ends, end_state, device_total = local_parts
    starts = jnp.cumsum(block_ends, axis=0) - block_ends
    full_states = before_local + jnp.exp(starts)[:, :, None, None] * state_in[None]
    cross = jnp.einsum(
        "nhid,nhde->nhie",
        decayed_queries,
        full_states.astype(jnp.bfloat16),
        preferred_element_type=jnp.float32,
    )
    output = intra_out + cross
    output = output * lax.rsqrt(jnp.mean(output * output, axis=-1, keepdims=True) + EPSILON)
    tok_rows = gate_proj.shape[0]
    output = jnp.transpose(output, (0, 2, 1, 3)).reshape(tok_rows, gate_proj.shape[1])
    return (output * jax.nn.silu(gate_proj.astype(jnp.float32))).astype(jnp.bfloat16)


def convolve(conv_proj, conv_kernel):
    gate_b, gate_c, conv_input = conv_proj
    tok_rows = gate_b.shape[0]
    product = gate_c.astype(jnp.float32) * conv_input.astype(jnp.float32)
    rim_rows = passed_along(product[tok_rows - (CONV_TAPS - 1) :], "sp", 1)
    padded = jnp.concatenate([rim_rows, product], axis=0)
    convolved = jnp.zeros_like(product)
    for tap_index in range(CONV_TAPS):
        convolved = convolved + conv_kernel[tap_index] * padded[tap_index : tap_index + tok_rows]
    return (gate_b.astype(jnp.float32) * convolved).astype(jnp.bfloat16)


def shards(
    tokens,
    norm_gain,
    query_weight,
    key_weight,
    value_weight,
    gate_weight,
    conv_b_weight,
    conv_c_weight,
    conv_in_weight,
    conv_kernel,
    out_ret_weight,
    out_conv_weight,
    log_decay,
):
    inputs = tokens[0].astype(jnp.float32)
    tok_rows = inputs.shape[0]
    normed = (
        inputs * lax.rsqrt(jnp.mean(inputs * inputs, axis=-1, keepdims=True) + EPSILON) * norm_gain
    ).astype(jnp.bfloat16)
    token_ordinal = (
        lax.axis_index("sp") * tok_rows + jnp.arange(tok_rows, dtype=jnp.int32)
    ).astype(jnp.float32)
    decays = log_decay[0]
    gathered = make_adder(
        normed,
        7,
        (
            lax.all_gather(query_weight, ("sp", "fs"), axis=0, tiled=True),
            lax.all_gather(key_weight, ("sp", "fs"), axis=0, tiled=True),
            lax.all_gather(value_weight, ("sp", "fs"), axis=0, tiled=True),
            lax.all_gather(gate_weight, ("sp", "fs"), axis=0, tiled=True),
            lax.all_gather(conv_b_weight, ("sp", "fs"), axis=0, tiled=True),
            lax.all_gather(conv_c_weight, ("sp", "fs"), axis=0, tiled=True),
            lax.all_gather(conv_in_weight, ("sp", "fs"), axis=0, tiled=True),
            lax.all_gather(out_ret_weight, ("sp", "fs"), axis=0, tiled=True),
            lax.all_gather(out_conv_weight, ("sp", "fs"), axis=0, tiled=True),
        ),
    )
    ret_proj = [member.astype(jnp.bfloat16) for member in gathered[:4]]
    local_parts = retention_local(ret_proj, decays, token_ordinal)
    state_in = carried(local_parts[4], local_parts[5])
    conv_proj = [member.astype(jnp.bfloat16) for member in gathered[4:7]]
    full_ret, full_conv = (gathered[7], gathered[8])
    conv_out = convolve(conv_proj, conv_kernel)
    ret_out = retention_finish(local_parts, state_in, ret_proj[3])
    partial_value = lax.dot_general(
        ret_out, full_ret, (((1,), (1,)), ((), ())), preferred_element_type=jnp.float32
    )
    mixed = lax.psum_scatter(
        (
            partial_value
            + lax.dot_general(
                conv_out, full_conv, (((1,), (1,)), ((), ())), preferred_element_type=jnp.float32
            )
        ).astype(jnp.bfloat16),
        "tp",
        scatter_dimension=0,
        tiled=True,
    )
    return mixed[None]


MESH_IDS = pl.DeviceIdType.MESH
WIDE_SHARE = 4


def remote(source, target, sent, landed, device):
    return pltpu.make_async_remote_copy(
        src_ref=source,
        dst_ref=target,
        send_sem=sent,
        recv_sem=landed,
        device_id=device,
        device_id_type=MESH_IDS,
    )


def greet(peers):
    barrier = pltpu.get_barrier_semaphore()
    for peer in peers:
        pl.semaphore_signal(barrier, inc=1, device_id=peer, device_id_type=MESH_IDS)
    pl.semaphore_wait(barrier, len(peers))


def plane_partners(f):
    x, y = f % 2, f // 2
    return y * 2 + (1 - x), (1 - y) * 2 + x, 3 - f


def mixer_kernel(
    n_sp,
    tokens_ref,
    gain_source,
    query_ref,
    key_ref,
    value_ref,
    gate_ref,
    conv_b_ref,
    conv_c_ref,
    conv_in_ref,
    taps_source,
    out_ret_ref,
    out_conv_ref,
    decay_source,
    near_cos_ref,
    near_sin_ref,
    base_source,
    out_ref,
    gain_ref,
    taps_ref,
    decay_ref,
    base_ref,
    raw_ref,
    normed_ref,
    pieces_ref,
    heads_ref,
    full_ref,
    outs_ref,
    decay_piece_ref,
    decays_ref,
    cos_ref,
    sin_ref,
    early_ref,
    proj_ref,
    intra_ref,
    decayed_ref,
    before_ref,
    starts_ref,
    product_ref,
    state_ref,
    extra_ref,
    state_piece_ref,
    states_ref,
    mixed_ref,
    merged_ref,
    part_ref,
    far_ref,
    local_sem,
    send_sem,
    full_landed,
    wide_landed,
    slim_landed,
    norm_landed,
    side_landed,
    state_landed,
    part_landed,
    once_landed,
):
    f32, bf16 = jnp.float32, jnp.bfloat16
    scope = jax.named_scope
    s, f, t = lax.axis_index("sp"), lax.axis_index("fs"), lax.axis_index("tp")
    xn, yn, dn = plane_partners(f)
    order = (xn, yn, dn)
    other = {"tp": 1 - t}
    n_fs, tok, model = normed_ref.shape
    half = tok // 2
    chunk = half // 2
    rows = query_ref.shape[0]
    slab_rows = n_fs * rows
    blocks = tok // BLOCK_LEN
    lanes = 2 * KEY_DIM
    pair = 2 * VALUE_DIM
    halo = CONV_TAPS - 1
    cut = rows * WIDE_SHARE // 8

    def lane(index, width):
        return pl.ds(pl.multiple_of(index * width, width), width)

    names = (
        "weight", "decay", "norm", "side", "relay", "up", "down", "wide", "wide_relay", "wide_up", "wide_down",
        "slim", "slim_relay", "slim_up", "slim_down", "state", "mixed", "part",
    )
    sent = {name: send_sem.at[i] for i, name in enumerate(names)}

    def all_sent(name, view):
        remote(view, view, sent[name], once_landed.at[0], other).wait_send()

    def line_sent(name, view_of):
        for i in range(n_sp - 1):
            here = i if name.endswith("up") else n_sp - 1 - i

            @pl.when(s == here)
            def _(i=i):
                all_sent(name, view_of(i + 1))

    def fetch(source, target, slot):
        copy = pltpu.make_async_copy(source, target, local_sem.at[slot])
        copy.start()
        return copy

    def fetched(view, slot):
        pltpu.make_async_copy(view, view, local_sem.at[slot]).wait()

    def own_rows(b, g):
        return pl.ds((b * n_fs + g) * rows, rows)

    def block(b, g):
        return full_ref.at[own_rows(b, g), :]

    def wide(b, g):
        return outs_ref.at[pl.ds((b * n_fs + g) * rows, cut), :]

    def wide_half(g, i):
        width = outs_ref.shape[1] // 2
        return outs_ref.at[pl.ds((s * n_fs + g) * rows, cut), pl.ds(i * width, width)]

    def slim(b, g):
        return outs_ref.at[pl.ds((b * n_fs + g) * rows + cut, rows - cut), :]

    fetch(query_ref, heads_ref.at[0], 0)
    fetch(key_ref, heads_ref.at[1], 0)
    fetch(decay_source, decay_ref, 8)
    wide_weights = (value_ref, gate_ref, conv_b_ref, conv_c_ref, conv_in_ref)
    for p in range(n_fs):
        for j, weight in enumerate(wide_weights):
            fetch(
                weight.at[:, pl.ds(p * VALUE_DIM, VALUE_DIM)],
                pieces_ref.at[p, :, pl.ds(lanes + j * VALUE_DIM, VALUE_DIM)],
                1,
            )
    for j, weight in enumerate(wide_weights):
        fetch(
            weight.at[:, lane(f, VALUE_DIM)],
            full_ref.at[own_rows(s, f), pl.ds(lanes + j * VALUE_DIM, VALUE_DIM)],
            2,
        )
    for i in range(2):
        fetch(
            tokens_ref.at[0, pl.ds(t * half + i * chunk, chunk), :],
            raw_ref.at[pl.ds(i * chunk, chunk), :],
            3 + i,
        )
    for g in range(n_fs):
        for j, weight in enumerate((out_ret_ref, out_conv_ref)):
            fetch(
                weight.at[:, pl.ds(g * VALUE_DIM, VALUE_DIM)],
                outs_ref.at[own_rows(s, f), pl.ds(g * pair + j * VALUE_DIM, VALUE_DIM)],
                5,
            )
    fetch(gain_source, gain_ref, 9)
    fetch(taps_source, taps_ref, 10)
    fetch(base_source, base_ref, 11)
    tables = [fetch(near_cos_ref, cos_ref, 6), fetch(near_sin_ref, sin_ref, 7)]

    with scope("greet"):
        peers = [{"fs": p} for p in order] + [other]
        peers += [{"sp": (s + d) % n_sp} for d in range(1, n_sp)]
        greet(peers)

    fetched(heads_ref, 0)
    for p in range(n_fs):
        own = pl.ds(p * KEY_DIM, KEY_DIM)
        pieces_ref[p, :, 0:lanes] = jnp.concatenate([heads_ref[0, :, own], heads_ref[1, :, own]], axis=-1)
    full_ref[own_rows(s, f), 0:lanes] = pieces_ref[f, :, 0:lanes]
    fetched(decay_ref, 8)
    decay_piece_ref[...] = jnp.zeros_like(decay_piece_ref)
    for p in range(n_fs):
        for n in range(blocks):
            decay_piece_ref[p, n : n + 1, :] = decay_ref[0, p : p + 1, n * BLOCK_LEN : (n + 1) * BLOCK_LEN]
    decays_ref[f] = decay_piece_ref[f]
    fetched(pieces_ref.at[:, :, lanes:], 1)
    for p in order:
        remote(pieces_ref.at[p], block(s, f), sent["weight"], full_landed.at[s, f], {"fs": p}).start()

    def line(view, up, down, landed):
        def copy(way):
            return remote(view, view, sent[up] if way == 1 else sent[down], landed, {"sp": s + way})

        def send():
            @pl.when(s < n_sp - 1)
            def _():
                copy(1).start()

            @pl.when(s > 0)
            def _():
                copy(-1).start()

        def step(way, there, then):
            further = (s < n_sp - 1) if way == 1 else (s > 0)

            @pl.when(there)
            def _():
                copy(way).wait_recv()

                @pl.when(further)
                def _():
                    copy(way).start()

                if then is not None:
                    then()

        return send, step

    def weight_line(b, g):
        return line(block(b, g), "up", "down", full_landed.at[b, g])

    def wide_line(b, g):
        return line(wide(b, g), "wide_up", "wide_down", wide_landed.at[b, g])

    def slim_line(b):
        return line(slim(b, f), "slim_up", "slim_down", slim_landed.at[b, f])

    def walk(make, d, then=None):
        for way in (1, -1):
            b = s - way * d
            there = (b >= 0) & (b <= n_sp - 1)
            b = jnp.where(there, b, s)
            make(b)[1](way, there, None if then is None else (lambda b=b: then(b)))

    fetched(full_ref.at[own_rows(s, f), lanes:], 2)
    weight_line(s, f)[0]()
    for p in order:
        remote(
            decay_piece_ref.at[p], decays_ref.at[f], sent["decay"], once_landed.at[1], {"fs": p}
        ).start()

    slab = 16

    def spot(owner, core, piece):
        return normed_ref.at[owner, pl.ds(core * half + piece * chunk, chunk), :]

    def normalise(piece):
        @pl.loop(0, chunk // slab)
        def _(i):
            x = raw_ref[pl.ds(piece * chunk + i * slab, slab), :].astype(f32)
            scale = lax.rsqrt(jnp.mean(x * x, axis=-1, keepdims=True) + EPSILON)
            normed_ref[f, pl.ds(t * half + piece * chunk + i * slab, slab), :] = (
                x * scale * gain_ref[...]
            ).astype(bf16)

    def norm_copy(owner, piece, kind, p):
        view = spot(owner, t, piece)
        return remote(view, view, sent[kind], norm_landed.at[owner, piece], {"fs": p})

    def side_copy(owner, piece):
        view = spot(owner, t, piece)
        remote(view, view, sent["side"], side_landed.at[owner], other).start()

    with scope("norm"):
        fetched(gain_ref, 9)
        fetched(raw_ref.at[0:chunk, :], 3)
        normalise(0)
        norm_copy(f, 0, "norm", xn).start()
        fetched(raw_ref.at[chunk:half, :], 4)
        normalise(1)
        norm_copy(f, 1, "norm", yn).start()
        norm_copy(f, 1, "norm", xn).start()
        norm_copy(f, 0, "norm", yn).start()
        for piece in range(2):
            side_copy(f, piece)

    with scope("w_plane"):
        for p in order:
            remote(pieces_ref.at[p], block(s, p), sent["weight"], full_landed.at[s, p], {"fs": p}).wait_recv()
            weight_line(s, p)[0]()
    fetched(outs_ref.at[own_rows(s, f), :], 5)
    for p in order[:2]:
        remote(wide(s, f), wide(s, f), sent["wide"], wide_landed.at[s, f], {"fs": p}).start()

    fetched(taps_ref, 10)
    fetched(base_ref, 11)
    for copy in tables:
        copy.wait()

    @pl.loop(0, blocks)
    def _(n):
        at = pl.ds(n * BLOCK_LEN, BLOCK_LEN)
        near_cos, near_sin = cos_ref[at, :], sin_ref[at, :]
        cos_ref[at, :] = near_cos * base_ref[0, pl.ds(s, 1), :] - near_sin * base_ref[1, pl.ds(s, 1), :]
        sin_ref[at, :] = near_sin * base_ref[2, pl.ds(s, 1), :] + near_cos * base_ref[3, pl.ds(s, 1), :]

    view = decay_piece_ref.at[0 : len(order)]
    remote(view, view, sent["decay"], once_landed.at[1], other).wait_recv()
    for g in range(n_fs):
        total = decays_ref[g]
        places = lax.broadcasted_iota(jnp.int32, total.shape, 1)
        shift = 1
        while shift < BLOCK_LEN:
            total = total + jnp.where(places >= shift, pltpu.roll(total, shift, 1), 0.0)
            shift *= 2
        decays_ref[g] = total

    def arrived(owner, piece):
        norm_copy(owner, piece, "norm", owner).wait_recv()
        side_copy(owner, piece)

    def side_arrived(owner):
        with scope("side"):
            view = normed_ref.at[owner, pl.ds((1 - t) * half, half), :]
            remote(view, view, sent["side"], side_landed.at[owner], other).wait_recv()

    def weight_step(d):
        with scope(f"w_line#d={d}"):
            for g in (f,) + order:
                walk(lambda b, g=g: weight_line(b, g), d)

    def nearest(k):
        ranked = [sorted(range(n_sp), key=lambda b: (abs(b - here), b))[k] for here in range(n_sp)]
        return sum(jnp.where(s == here, b, 0) for here, b in enumerate(ranked))

    def columns(o, at, b):
        return jnp.dot(
            normed_ref[o, at, lane(b, slab_rows)],
            full_ref[pl.ds(pl.multiple_of(b * slab_rows, slab_rows), slab_rows), :],
            preferred_element_type=f32,
        )

    def project_early(o, i):
        side_arrived(o)
        with scope("early"):
            near = [nearest(k) for k in range(n_sp - 1)]

            @pl.loop(0, tok // chunk)
            def _(j):
                at = pl.ds(j * chunk, chunk)
                early_ref[i, at, :] = sum(columns(o, at, b) for b in near)

    def project_late(o, i):
        with scope("late"):
            last = nearest(n_sp - 1)

            @pl.loop(0, tok // chunk)
            def _(j):
                at = pl.ds(j * chunk, chunk)
                proj_ref[o, at, :] = (early_ref[i, at, :] + columns(o, at, last)).astype(bf16)

    def project(o):
        side_arrived(o)
        with scope("project"):

            @pl.loop(0, tok // chunk)
            def _(j):
                at = pl.ds(j * chunk, chunk)
                proj_ref[o, at, :] = jnp.dot(
                    normed_ref[o, at, :], full_ref[...], preferred_element_type=f32
                ).astype(bf16)

    weight_step(1)
    with scope("x_first"):
        arrived(xn, 0)
        norm_copy(xn, 0, "relay", yn).start()
        arrived(yn, 1)
        norm_copy(yn, 1, "relay", xn).start()
    for d in range(2, n_sp - 1):
        weight_step(d)
    slim_line(s)[0]()
    wide_line(s, f)[0]()
    project_early(f, 0)
    with scope("x_second"):
        arrived(xn, 1)
        arrived(yn, 0)

    with scope("wide_plane"):
        for i, p in enumerate(order[:2]):
            remote(wide(s, p), wide(s, p), sent["wide"], wide_landed.at[s, p], {"fs": p}).wait_recv()
            view = wide_half(p, i)
            remote(view, view, sent["wide_relay"], wide_landed.at[s, p], {"fs": order[1 - i]}).start()

    def wide_far():
        with scope("wide_far"):
            remote(wide(s, dn), wide(s, dn), sent["wide"], wide_landed.at[s, dn], {"fs": dn}).wait_recv()

    def slim_spread(b):
        for p in order[:2]:
            remote(slim(b, f), slim(b, f), sent["slim"], slim_landed.at[b, f], {"fs": p}).start()

    def slim_arrived(b, g):
        remote(slim(b, g), slim(b, g), sent["slim"], slim_landed.at[b, g], {"fs": g}).wait_recv()

    def at_distance(d):
        for way in (1, -1) if d else (1,):
            b = s - way * d
            there = (b >= 0) & (b <= n_sp - 1)
            yield jnp.where(there, b, s), there

    def slim_plane(d):
        for b, there in at_distance(d):
            pl.when(there)(lambda b=b: slim_spread(b))

    def slim_relay(d):
        with scope(f"relay#d={d}"):
            for b, there in at_distance(d):
                near = b < n_sp // 2
                first, onward = jnp.where(near, xn, yn), jnp.where(near, yn, xn)

                @pl.when(there)
                def _():
                    slim_arrived(b, first)
                    view = slim(b, first)
                    remote(view, view, sent["slim_relay"], slim_landed.at[b, first], {"fs": onward}).start()

    def slim_rest(d):
        for b, there in at_distance(d):

            @pl.when(there)
            def _():
                slim_arrived(b, jnp.where(b < n_sp // 2, yn, xn))
                slim_arrived(b, dn)

    def slim_step(d):
        with scope(f"slim#d={d}"):
            walk(slim_line, d)

    def wide_step(d, g):
        with scope(f"wide#d={d}"):
            walk(lambda b: wide_line(b, g), d)

    def part(o, at, index):
        return proj_ref[o, at, lanes + index * VALUE_DIM : lanes + (index + 1) * VALUE_DIM]

    causal = lax.broadcasted_iota(jnp.int32, (BLOCK_LEN, BLOCK_LEN), 0) >= lax.broadcasted_iota(
        jnp.int32, (BLOCK_LEN, BLOCK_LEN), 1
    )
    front = lax.broadcasted_iota(jnp.int32, (BLOCK_LEN, lanes), 1) % KEY_DIM < KEY_DIM // 2

    def rounded(x):
        return x.astype(bf16).astype(f32)

    def retain(o):
        def body(n, carry):
            state, total = carry
            at = pl.ds(pl.multiple_of(n * BLOCK_LEN, BLOCK_LEN), BLOCK_LEN)
            row = decays_ref[o, pl.ds(n, 1), :]
            end = jnp.broadcast_to(row[:, BLOCK_LEN - 1 :], row.shape)
            across = jnp.broadcast_to(row, (BLOCK_LEN, BLOCK_LEN))
            down = across.T
            weighting = jnp.where(causal, jnp.exp(jnp.minimum(down - across, 0.0)), 0.0)
            x = proj_ref[o, at, 0:lanes].astype(f32)
            swapped = jnp.where(
                front, pltpu.roll(x, lanes - KEY_DIM // 2, 1), pltpu.roll(x, KEY_DIM // 2, 1)
            )
            turned = (x * cos_ref[at, :] + swapped * sin_ref[at, :]).astype(bf16)
            queries = turned[:, :KEY_DIM]
            keys = turned.astype(f32).T[KEY_DIM:, :]
            values = part(o, at, 0)
            raw = jnp.dot(queries, keys.astype(bf16), preferred_element_type=f32)
            scores = (raw * weighting).astype(bf16)
            intra_ref[o, at, :] = jnp.dot(scores, values, preferred_element_type=f32)
            decayed_ref[o, at, :] = (queries.astype(f32) * jnp.exp(down[:, :KEY_DIM])).astype(bf16)
            late = (keys * jnp.exp(end - row)).astype(bf16)
            before_ref[o, n] = state
            starts_ref[o, pl.ds(n, 1), :] = total
            product_ref[o, pl.ds(pl.multiple_of(8 + n * BLOCK_LEN, 8), BLOCK_LEN), :] = part(o, at, 3).astype(
                f32
            ) * part(o, at, 4).astype(f32)
            state = state * jnp.exp(end) + jnp.dot(late, values, preferred_element_type=f32)
            return state, total + end

        with scope("retain"):
            state, total = lax.fori_loop(
                0, blocks, body, (jnp.zeros((KEY_DIM, VALUE_DIM), f32), jnp.zeros((1, VALUE_DIM), f32))
            )
            rim = product_ref[o, 8 + tok - halo : 8 + tok, :]
            middle = total - rounded(total)
            extra_ref[...] = jnp.zeros_like(extra_ref)
            extra_ref[0:halo, :] = rounded(rim)
            extra_ref[halo : 2 * halo, :] = rim - rounded(rim)
            extra_ref[8:9, :] = rounded(total)
            extra_ref[9:10, :] = rounded(middle)
            extra_ref[10:11, :] = middle - rounded(middle)
            state_piece_ref[o, 0:KEY_DIM, :] = state.astype(bf16)
            state_piece_ref[o, KEY_DIM:, :] = extra_ref[...].astype(bf16)
            for d in range(1, n_sp):

                @pl.when(s + d < n_sp)
                def _():
                    state_copy(o, s, d).start()

    def state_copy(o, owner, d):
        return remote(
            state_piece_ref.at[o],
            states_ref.at[owner, o],
            sent["state"],
            state_landed.at[owner, o],
            {"sp": (s + d) % n_sp},
        )

    def finish(o, put):
        with scope("state"):
            state_ref[...] = jnp.zeros_like(state_ref)
            product_ref[o, 0:8, :] = jnp.zeros((8, VALUE_DIM), f32)
            for k in range(n_sp - 1):

                @pl.when(k < s)
                def _():
                    state_copy(o, k, 1).wait_recv()
                    extra_ref[...] = states_ref[k, o, KEY_DIM:, :].astype(f32)
                    total = extra_ref[8:9, :] + extra_ref[9:10, :] + extra_ref[10:11, :]
                    state_ref[...] = state_ref[...] * jnp.exp(total) + states_ref[k, o, 0:KEY_DIM, :].astype(f32)

                @pl.when(k == s - 1)
                def _():
                    product_ref[o, 8 - halo : 8, :] = extra_ref[0:halo, :] + extra_ref[halo : 2 * halo, :]

        taps = [taps_ref[k : k + 1, lane(f, VALUE_DIM)] for k in range(CONV_TAPS)]
        with scope("finish"):

            @pl.loop(0, blocks)
            def _(n):
                at = pl.ds(pl.multiple_of(n * BLOCK_LEN, BLOCK_LEN), BLOCK_LEN)
                state = before_ref[o, n] + jnp.exp(starts_ref[o, pl.ds(n, 1), :]) * state_ref[...]
                output = intra_ref[o, at, :] + jnp.dot(
                    decayed_ref[o, at, :], state.astype(bf16), preferred_element_type=f32
                )
                output = output * lax.rsqrt(jnp.mean(output * output, axis=-1, keepdims=True) + EPSILON)
                gate = part(o, at, 1).astype(f32)
                ret_out = (output * (gate / (1.0 + jnp.exp(-gate)))).astype(bf16)
                padded = product_ref[o, pl.ds(pl.multiple_of(n * BLOCK_LEN, 8), BLOCK_LEN + 8), :]
                convolved = sum(
                    taps[k] * padded[8 - halo + k : 8 - halo + k + BLOCK_LEN, :] for k in range(CONV_TAPS)
                )
                conv_out = (part(o, at, 2).astype(f32) * convolved).astype(bf16)
                put(at, ret_out, conv_out)

    def mixed_out(o, i):
        def put(at, ret_out, conv_out):
            mixed_ref[i, at, 0:VALUE_DIM] = ret_out
            mixed_ref[i, at, VALUE_DIM:pair] = conv_out

        finish(o, put)
        remote(
            mixed_ref.at[i], merged_ref.at[:, lane(f, pair)], sent["mixed"], once_landed.at[2], {"fs": o}
        ).start()

    def keep(at, ret_out, conv_out):
        merged_ref[at, lane(2 * f, VALUE_DIM)] = ret_out
        merged_ref[at, lane(2 * f + 1, VALUE_DIM)] = conv_out

    middle = range(2, n_sp - 1)
    slim_plane(0)
    project_early(xn, 1)
    project_early(yn, 2)
    weight_step(n_sp - 1)
    project_late(xn, 1)
    retain(xn)
    slim_step(1)
    slim_plane(1)
    wide_line(s, xn)[0]()
    project_late(yn, 2)
    retain(yn)
    for d in middle:
        slim_step(d)
        slim_plane(d)
    wide_step(1, f)
    mixed_out(xn, 0)
    mixed_out(yn, 1)
    wide_step(1, xn)
    with scope("x_third"):
        arrived(dn, 0)
        arrived(dn, 1)
    project(dn)
    slim_relay(0)
    slim_step(n_sp - 1)
    retain(dn)
    wide_far()
    wide_line(s, yn)[0]()
    wide_line(s, dn)[0]()
    project_late(f, 0)
    for d in middle:
        wide_step(d, f)
    slim_relay(1)
    mixed_out(dn, 2)
    slim_plane(n_sp - 1)
    for d in middle:
        wide_step(d, xn)
    retain(f)
    for d in middle:
        slim_relay(d)
    wide_step(1, yn)
    finish(f, keep)
    wide_step(1, dn)
    for d in middle:
        wide_step(d, yn)
        wide_step(d, dn)
    with scope("settle"):
        all_sent("weight", pieces_ref.at[0 : len(order)])
        all_sent("decay", decay_piece_ref.at[0 : len(order)])
        all_sent("norm", normed_ref.at[0])
        all_sent("relay", normed_ref.at[0, 0:half, :])
        all_sent("side", normed_ref.at[0:2])
        all_sent("wide", outs_ref.at[0 : 2 * cut, :])
        all_sent("wide_relay", outs_ref.at[0:cut, :])
        for way in ("up", "down"):
            line_sent(way, lambda k: full_ref.at[0 : k * slab_rows, :])
            line_sent("slim_" + way, lambda k: outs_ref.at[0 : k * (rows - cut), :])
        for k in range(1, n_sp):

            @pl.when(s == n_sp - 1 - k)
            def _(k=k):
                all_sent("state", states_ref.at[0:k])

    with scope("h_wait"):
        view = merged_ref.at[:, 0 : len(order) * pair]
        remote(view, view, sent["mixed"], once_landed.at[2], other).wait_recv()

    def part_copy(b):
        return remote(part_ref.at[0, b], far_ref.at[b], sent["part"], part_landed.at[b], other)

    def out_tile(b):
        @pl.loop(0, 2)
        def _(j):
            core = jnp.where(j == 0, 1 - t, t)
            part_ref[j, b] = lax.dot_general(
                merged_ref[pl.ds(pl.multiple_of(core * half, half), half), :],
                outs_ref[pl.ds(pl.multiple_of(b * slab_rows, slab_rows), slab_rows), :],
                (((1,), (1,)), ((), ())),
                preferred_element_type=f32,
            ).astype(bf16)

            @pl.when(j == 0)
            def _():
                part_copy(b).start()

    def out_sum(k):
        with scope("o_sum"):
            b = nearest(k)
            part_copy(b).wait_recv()
            out_ref[:, lane(b, slab_rows)] = (part_ref[1, b].astype(f32) + far_ref[b].astype(f32)).astype(bf16)

    for k in range(n_sp):
        if k == 1:
            slim_relay(n_sp - 1)
        with scope(f"o_wait#k={k}"):
            if k == n_sp - 1:
                for g in (f,) + order:
                    wide_step(k, g)
            slim_rest(k)
        with scope(f"o_tile#k={k}"):
            out_tile(nearest(k))
        if k > 0:
            out_sum(k - 1)
    with scope("o_settle"):
        for way in ("up", "down"):
            line_sent("wide_" + way, lambda k: outs_ref.at[0 : k * n_fs * cut, :])
        all_sent("slim", outs_ref.at[0 : 2 * n_sp * (rows - cut), :])
        all_sent("slim_relay", outs_ref.at[0 : n_sp * (rows - cut), :])
        all_sent("mixed", mixed_ref)
        all_sent("part", far_ref)
    out_sum(n_sp - 1)


def fast_shards(
    tokens,
    norm_gain,
    query_weight,
    key_weight,
    value_weight,
    gate_weight,
    conv_b_weight,
    conv_c_weight,
    conv_in_weight,
    conv_kernel,
    out_ret_weight,
    out_conv_weight,
    log_decay,
):
    n_sp, n_fs = lax.axis_size("sp"), lax.axis_size("fs")
    tok, model = tokens.shape[1:]
    half = tok // 2
    blocks = tok // BLOCK_LEN
    rows = query_weight.shape[0]
    width = 2 * KEY_DIM + 5 * VALUE_DIM
    lanes, pair = 2 * KEY_DIM, 2 * VALUE_DIM

    frequency = np.tile(1.0 / ROPE_BASE ** np.linspace(0.0, 1.0, KEY_DIM // 2), 4)
    near = np.arange(tok)[:, None] * frequency[None, :]
    far = (np.arange(n_sp) * tok)[:, None] * frequency[None, :]
    scale = np.where(np.arange(lanes) < KEY_DIM, 1.0, KEY_DIM ** (-0.5))
    sign = np.where(np.arange(lanes) % KEY_DIM < KEY_DIM // 2, -1.0, 1.0)
    base = np.stack(
        [np.cos(far) * scale, np.sin(far) * scale, np.cos(far) * scale * sign, np.sin(far) * scale * sign]
    )

    any_space = pl.BlockSpec(memory_space=pl.ANY)
    vmem = pl.BlockSpec(memory_space=pltpu.VMEM)
    dma = pltpu.SemaphoreType.DMA
    f32, bf16 = jnp.float32, jnp.bfloat16
    buffers = [
        ((1, model), f32),
        (conv_kernel.shape, f32),
        (log_decay.shape, f32),
        (base.shape, f32),
        ((half, model), bf16),
        ((n_fs, tok, model), bf16),
        ((n_fs, rows, width), bf16),
        ((2, rows, n_fs * KEY_DIM), bf16),
        ((n_sp * n_fs * rows, width), bf16),
        ((n_sp * n_fs * rows, n_fs * pair), bf16),
        ((n_fs, 8, BLOCK_LEN), f32),
        ((n_fs, 8, BLOCK_LEN), f32),
        ((tok, lanes), f32),
        ((tok, lanes), f32),
        ((n_fs - 1, tok, width), f32),
        ((n_fs, tok, width), bf16),
        ((n_fs, tok, VALUE_DIM), f32),
        ((n_fs, tok, KEY_DIM), bf16),
        ((n_fs, blocks, KEY_DIM, VALUE_DIM), f32),
        ((n_fs, 8, VALUE_DIM), f32),
        ((n_fs, 8 + tok, VALUE_DIM), f32),
        ((KEY_DIM, VALUE_DIM), f32),
        ((16, VALUE_DIM), f32),
        ((n_fs, KEY_DIM + 16, VALUE_DIM), bf16),
        ((n_sp, n_fs, KEY_DIM + 16, VALUE_DIM), bf16),
        ((n_fs - 1, tok, pair), bf16),
        ((tok, n_fs * pair), bf16),
        ((2, n_sp, half, n_fs * rows), bf16),
        ((n_sp, half, n_fs * rows), bf16),
    ]
    semaphores = [
        (12,),
        (18,),
        (n_sp, n_fs),
        (n_sp, n_fs),
        (n_sp, n_fs),
        (n_fs, 2),
        (n_fs,),
        (n_sp, n_fs),
        (n_sp,),
        (3,),
    ]
    operands = (
        tokens,
        norm_gain.reshape(1, model),
        query_weight,
        key_weight,
        value_weight,
        gate_weight,
        conv_b_weight,
        conv_c_weight,
        conv_in_weight,
        conv_kernel,
        out_ret_weight,
        out_conv_weight,
        log_decay,
        jnp.asarray(np.cos(near), jnp.float32),
        jnp.asarray(np.sin(near), jnp.float32),
        jnp.asarray(base, jnp.float32),
    )
    mixed = pl.pallas_call(
        lambda *refs: mixer_kernel(n_sp, *refs),
        out_shape=jax.ShapeDtypeStruct((half, model), bf16),
        in_specs=[any_space] * len(operands),
        out_specs=vmem,
        scratch_shapes=[pltpu.VMEM(shape, kind) for shape, kind in buffers] + [dma(shape) for shape in semaphores],
        compiler_params=pltpu.CompilerParams(
            collective_id=0, has_side_effects=True, vmem_limit_bytes=50 * 1024 * 1024
        ),
        name="mixer",
    )(*(pltpu.with_memory_space_constraint(x, pltpu.HBM) for x in operands))
    return mixed[None]


def select(mesh):
    def chosen(*arrays):
        heads, conv_width = arrays[12].shape[1], arrays[9].shape[1]
        n_sp, n_fs, n_tp = (mesh.shape[name] for name in ("sp", "fs", "tp"))
        tok, model = arrays[0].shape[1:]
        fits = n_fs == 4 and n_tp == 2 and n_sp > 2 and heads == n_fs
        fits = fits and conv_width == n_fs * VALUE_DIM and tok % (2 * BLOCK_LEN) == 0
        fits = fits and tok // BLOCK_LEN <= 8 and arrays[10].shape[0] % BLOCK_LEN == 0
        return (fast_shards if fits else shards)(*arrays)

    return chosen


def solution(mesh):
    in_specs = (
        P("fs", "sp", None),
        P(),
        P(("sp", "fs"), "tp"),
        P(("sp", "fs"), "tp"),
        P(("sp", "fs"), "tp"),
        P(("sp", "fs"), "tp"),
        P(("sp", "fs"), "tp"),
        P(("sp", "fs"), "tp"),
        P(("sp", "fs"), "tp"),
        P(None, "tp"),
        P(("sp", "fs"), "tp"),
        P(("sp", "fs"), "tp"),
        P("fs", "tp", "sp"),
    )
    out_specs = P("fs", ("sp", "tp"), None)
    return jax.shard_map(select(mesh), mesh=mesh, in_specs=in_specs, out_specs=out_specs, check_vma=False)
```
